32 devices in a mesh: sp: 8 (over z, y), tp: 4 (over x, core).
Axes of the slice: x: 2, y: 2, z: 4, core: 2. Of those that a mesh axis runs over, the one named last changes fastest.
Arguments:
- inputs: bfloat16 [2, 1024, 2048], P(None, 'sp'), may hold values from -6 to 6
- norm_gain: float32 [2048], replicated, may hold values from 0.1 to 1.9
- query_weight: bfloat16 [2048, 1024], P('sp', 'tp'), may hold values from -0.125 to 0.125
- key_weight: bfloat16 [2048, 256], P('sp', 'tp'), may hold values from -0.125 to 0.125
- value_weight: bfloat16 [2048, 256], P('sp', 'tp'), may hold values from -0.125 to 0.125
- query_gain: float32 [64], replicated, may hold values from 0.1 to 24
- key_gain: float32 [64], replicated, may hold values from 0.1 to 1.9
- forget_cache: float32 [2, 16, 1024], P(None, 'tp'), may hold values from -104 to 0, as said below
- rec_in_weight: bfloat16 [2048, 1024], P('sp', 'tp'), may hold values from -0.125 to 0.125
- rec_gate_weight: bfloat16 [2048, 1024], P('sp', 'tp'), may hold values from -0.125 to 0.125
- conv_weight: bfloat16 [4, 1024], P(None, 'tp'), may hold values from -3 to 3
- decay_gate_weight: bfloat16 [16, 64, 64], P('tp'), may hold values from -0.75 to 0.75
- input_gate_weight: bfloat16 [16, 64, 64], P('tp'), may hold values from -0.75 to 0.75
- decay_param: float32 [1024], P('tp'), may hold values from 4 to 16
- decay_extra: float32 [2, 1024, 1024], P(None, 'sp', 'tp'), may hold values from -2 to 0
- attn_out_gain: float32 [1024], P('tp'), may hold values from 0.1 to 1.9
- rec_out_gain: float32 [1024], P('tp'), may hold values from 0.1 to 1.9
- out_att_weight: bfloat16 [1024, 2048], P('tp'), may hold values from -0.125 to 0.125
- out_rec_weight: bfloat16 [1024, 2048], P('tp'), may hold values from -0.125 to 0.125
Outputs:
- mixed: bfloat16 [2, 1024, 2048], P(None, 'sp', 'tp')
The draws below stay inside these ranges and needn't reach their ends.
Inputs may be any that keep to these rules, and one draw needn't show every extreme that they name: `forget_cache`: Non-increasing along the positions of each sequence and head.
All inputs are finite; a program needn't handle non-finite values.
Results may differ from the reference program's by a relative error of at most 0.012.
The reference program's roundings to bfloat16 on the way count: a program that leaves them out, or rounds other values in their place, can miss the bound.
Values may be sent and summed in bfloat16 or wider, within the bound.
No kernel may reach another device: no remote copies, remote signals or barrier semaphores. Data moves between devices by JAX's collectives and lax.ppermute only.
A program may use at most 128 MiB of HBM per device.

```python
import math
import jax
import jax.numpy as jnp
from jax import lax

D = 2048
HEAD_DIM = 64
ATT_HEADS = 16
KV_HEADS = 4
LRU_BLOCK = 64
CONV_TAPS = 4
SEQS = 2
SEQ_TOK = 128
SEQUENCE_LENGTH = 1024
ATT_WIDTH = 1024
KV_WIDTH = 256
LRU_WIDTH = 1024
LRU_BLOCKS = 16


lru_const = 8.0


def spike_log_values(key, total_count):
    key_rows = jax.random.split(key, 2)
    spots = jax.random.randint(key_rows[0], (SEQS, total_count), 0, SEQUENCE_LENGTH)
    kept = jax.random.uniform(key_rows[1], (SEQS, total_count), jnp.float32, 0.5, 0.8)
    hits = (jnp.arange(SEQUENCE_LENGTH)[None, None, :] == spots[:, :, None]).astype(jnp.float32)
    return jnp.sum(hits * jnp.log(kept)[:, :, None], axis=1)


def block_factor(key):
    blocks = SEQUENCE_LENGTH // SEQ_TOK
    multiplier = jnp.exp(jax.random.uniform(key, (SEQS, blocks), jnp.float32, math.log(0.5), math.log(2.0)))
    return jnp.repeat(multiplier, SEQ_TOK, axis=1)


def draw_query_gain(key, part):
    key = jax.random.fold_in(key, 3)
    return 1.0 + 0.18 * jnp.clip(jax.random.normal(key, (HEAD_DIM,), jnp.float32), -4.5, 4.5)


def draw_forget_cache(key, part):
    key_rows = jax.random.split(jax.random.fold_in(key, 7), 6)
    order = jax.random.permutation(key_rows[0], ATT_HEADS)
    slow_rate = 0.6 / SEQUENCE_LENGTH * jax.random.uniform(key_rows[1], (ATT_HEADS,), jnp.float32, 0.5, 1.5)
    fast_len = jnp.exp(jax.random.uniform(key_rows[2], (ATT_HEADS,), jnp.float32, math.log(30.0), math.log(100.0)))
    decay_speed = jnp.where(order < ATT_HEADS // 2, 1.0 / fast_len, slow_rate)
    random_jitter = jax.random.uniform(key_rows[4], (SEQS, ATT_HEADS, SEQUENCE_LENGTH), jnp.float32, 0.5, 1.5)
    multiplier = block_factor(key_rows[3])
    gate_logarithm = -decay_speed[None, :, None] * multiplier[:, None, :] * random_jitter + spike_log_values(key_rows[5], 2)[:, None, :]
    return jnp.cumsum(gate_logarithm, axis=2)


def draw_decay_param(key, part):
    key_rows = jax.random.split(jax.random.fold_in(key, 5), 3)
    order = jax.random.permutation(key_rows[0], LRU_WIDTH)
    slow_rate = 0.3 / (lru_const * SEQUENCE_LENGTH) * jax.random.uniform(key_rows[1], (LRU_WIDTH,), jnp.float32, 0.5, 1.5)
    fast_len = jnp.exp(jax.random.uniform(key_rows[2], (LRU_WIDTH,), jnp.float32, math.log(30.0), math.log(100.0)))
    fast_rate = 1.0 / (0.5 * lru_const * fast_len)
    decay_speed = jnp.where(order < LRU_WIDTH // 2, fast_rate, slow_rate)
    return -jnp.log(jnp.expm1(decay_speed))


def draw_decay_extra(key, part):
    key_rows = jax.random.split(jax.random.fold_in(key, 9), 3)
    multiplier = block_factor(key_rows[0])
    random_jitter = jax.random.uniform(key_rows[1], (SEQS, SEQUENCE_LENGTH, LRU_WIDTH), jnp.float32, 0.5, 1.5)
    return -0.5 / SEQUENCE_LENGTH * multiplier[:, :, None] * random_jitter + spike_log_values(key_rows[2], 2)[:, :, None]


def block_scale(stream_key, dims, pieces, low, largest):
    loudness, own = 1.0, jax.random.fold_in(stream_key, 6)
    for dim, shards_of in pieces:
        draws = jnp.exp(jax.random.uniform(jax.random.fold_in(own, dim), (shards_of,), jnp.float32, low / len(pieces), largest / len(pieces)))
        loudness = loudness * jnp.repeat(draws, dims[dim] // shards_of).reshape([-1 if axis == dim else 1 for axis in range(len(dims))])
    return loudness


def normal_values(stream_key, extent, width, limit, shards=(), kind=jnp.bfloat16):
    result = width * jax.random.normal(stream_key, extent, jnp.float32)
    if shards:
        result = result * block_scale(stream_key, extent, shards, -0.22, 0.18)
    return jnp.clip(result, -limit, limit).astype(kind)


def setup_inputs(seed: int = 0) -> dict:
    key_of = jax.random.split(jax.random.key(seed), 20)
    inputs = normal_values(key_of[0], (SEQS, SEQUENCE_LENGTH, D), 1.0, 6.0, ((1, 8),))
    norm_gain = jnp.clip(1.0 + 0.18 * jax.random.normal(key_of[1], (D,), jnp.float32), 0.1, 1.9)
    query_weight = normal_values(key_of[2], (D, ATT_WIDTH), D ** -0.5, 0.125, ((0, 8), (1, 4)))
    key_weight = normal_values(key_of[3], (D, KV_WIDTH), D ** -0.5, 0.125, ((0, 8), (1, 4)))
    value_weight = normal_values(key_of[4], (D, KV_WIDTH), D ** -0.5, 0.125, ((0, 8), (1, 4)))
    query_gain = draw_query_gain(jax.random.fold_in(key_of[19], 71), 0)
    key_gain = jnp.clip(1.0 + 0.18 * jax.random.normal(key_of[6], (HEAD_DIM,), jnp.float32), 0.1, 1.9)
    forget_cache = draw_forget_cache(jax.random.fold_in(key_of[19], 71), 0)
    rec_in_weight = normal_values(key_of[8], (D, LRU_WIDTH), D ** -0.5, 0.125, ((0, 8), (1, 4)))
    rec_gate_weight = normal_values(key_of[9], (D, LRU_WIDTH), D ** -0.5, 0.125, ((0, 8), (1, 4)))
    conv_weight = normal_values(key_of[10], (CONV_TAPS, LRU_WIDTH), CONV_TAPS ** -0.5, 3.0, ((1, 4),))
    decay_gate_weight = normal_values(key_of[11], (LRU_BLOCKS, LRU_BLOCK, LRU_BLOCK), LRU_BLOCK ** -0.5, 0.75, ((0, 4),))
    input_gate_weight = normal_values(key_of[12], (LRU_BLOCKS, LRU_BLOCK, LRU_BLOCK), LRU_BLOCK ** -0.5, 0.75, ((0, 4),))
    decay_param = draw_decay_param(jax.random.fold_in(key_of[19], 71), 0)
    decay_extra = draw_decay_extra(jax.random.fold_in(key_of[19], 71), 0)
    attn_out_gain = jnp.clip(1.0 + 0.18 * jax.random.normal(key_of[15], (ATT_WIDTH,), jnp.float32), 0.1, 1.9)
    rec_out_gain = jnp.clip(1.0 + 0.18 * jax.random.normal(key_of[16], (LRU_WIDTH,), jnp.float32), 0.1, 1.9)
    out_att_weight = normal_values(key_of[17], (ATT_WIDTH, D), D ** -0.5, 0.125, ((0, 4),))
    out_rec_weight = normal_values(key_of[18], (LRU_WIDTH, D), D ** -0.5, 0.125, ((0, 4),))
    return {"inputs": inputs, "norm_gain": norm_gain, "query_weight": query_weight, "key_weight": key_weight, "value_weight": value_weight, "query_gain": query_gain, "key_gain": key_gain, "forget_cache": forget_cache, "rec_in_weight": rec_in_weight, "rec_gate_weight": rec_gate_weight, "conv_weight": conv_weight, "decay_gate_weight": decay_gate_weight, "input_gate_weight": input_gate_weight, "decay_param": decay_param, "decay_extra": decay_extra, "attn_out_gain": attn_out_gain, "rec_out_gain": rec_out_gain, "out_att_weight": out_att_weight, "out_rec_weight": out_rec_weight}


lru_const = 8.0
norm_eps = 1e-06

def rms_scale(values, gain):
    multiplier = lax.rsqrt(lax.optimization_barrier(jnp.mean(values * values, axis=-1, keepdims=True)) + norm_eps)
    return values * multiplier * gain

def merge_state(earlier, later):
    return (earlier[0] * later[0], later[0] * earlier[1] + later[1])

def attention(queries, key_heads, value_heads, forget_cache):
    seq_count, kv_count, head_group, length, head_dim = queries.shape
    block_size = 512
    while length % block_size:
        block_size //= 2
    scaling = head_dim ** (-0.5)
    gates = forget_cache.reshape(seq_count, kv_count, head_group, length)
    offsets = jnp.arange(block_size, dtype=jnp.int32)

    def one_block(index):
        first = index * block_size
        query_block = lax.dynamic_slice_in_dim(queries, first, block_size, 3).astype(jnp.float32)
        query_gates = lax.dynamic_slice_in_dim(gates, first, block_size, 3)
        query_pos = first + offsets

        def one_step(block_index, carried):
            top_score, totals, accum = carried
            key_first = block_index * block_size
            key_block = lax.dynamic_slice_in_dim(key_heads, key_first, block_size, 2).astype(jnp.float32)
            value_block = lax.dynamic_slice_in_dim(value_heads, key_first, block_size, 2).astype(jnp.float32)
            key_gates = lax.dynamic_slice_in_dim(gates, key_first, block_size, 3)
            scores = jnp.einsum('bhgqd,bhkd->bhgqk', query_block, key_block) * scaling
            scores = scores + query_gates[..., :, None] - key_gates[..., None, :]
            visible = query_pos[:, None] >= (key_first + offsets)[None, :]
            scores = jnp.where(visible, scores, -jnp.inf)
            new_top = jnp.maximum(top_score, lax.optimization_barrier(jnp.max(scores, axis=-1)))
            weights = jnp.exp(scores - new_top[..., None])
            fading = jnp.exp(top_score - new_top)
            rounded = lax.optimization_barrier(weights.astype(jnp.bfloat16)).astype(jnp.float32)
            totals = totals * fading + lax.optimization_barrier(jnp.sum(weights, axis=-1))
            accum = accum * fading[..., None] + jnp.einsum('bhgqk,bhkd->bhgqd', rounded, value_block)
            return (new_top, totals, accum)
        start_state = (jnp.full((seq_count, kv_count, head_group, block_size), -jnp.inf, jnp.float32), jnp.zeros((seq_count, kv_count, head_group, block_size), jnp.float32), jnp.zeros((seq_count, kv_count, head_group, block_size, head_dim), jnp.float32))
        top_score, totals, accum = lax.fori_loop(0, index + 1, one_step, start_state)
        return accum / totals[..., None]
    return lax.map(one_block, jnp.arange(length // block_size, dtype=jnp.int32))

def reference(inputs, norm_gain, query_weight, key_weight, value_weight, query_gain, key_gain, forget_cache, rec_in_weight, rec_gate_weight, conv_weight, decay_gate_weight, input_gate_weight, decay_param, decay_extra, attn_out_gain, rec_out_gain, out_att_weight, out_rec_weight):
    seq_count, length, model_width = inputs.shape
    row_count = seq_count * length
    head_group = ATT_HEADS // KV_HEADS
    flat_rows = inputs.reshape(row_count, model_width).astype(jnp.float32)
    normed = rms_scale(flat_rows, norm_gain).astype(jnp.bfloat16)

    def project(weight):
        return jnp.dot(normed, weight, preferred_element_type=jnp.float32)
    query_proj = project(query_weight)
    key_proj = project(key_weight)
    gate_proj = project(rec_gate_weight)
    value_proj = project(value_weight).astype(jnp.bfloat16)
    rec_in = project(rec_in_weight).astype(jnp.bfloat16)
    queries = rms_scale(query_proj.reshape(seq_count, length, ATT_HEADS, HEAD_DIM), query_gain).astype(jnp.bfloat16)
    queries = queries.transpose(0, 2, 1, 3).reshape(seq_count, KV_HEADS, head_group, length, HEAD_DIM)
    key_heads = rms_scale(key_proj.reshape(seq_count, length, KV_HEADS, HEAD_DIM), key_gain).astype(jnp.bfloat16)
    key_heads = key_heads.transpose(0, 2, 1, 3)
    value_heads = value_proj.reshape(seq_count, length, KV_HEADS, HEAD_DIM).transpose(0, 2, 1, 3)
    blocks = attention(queries, key_heads, value_heads, forget_cache)
    attended = blocks.transpose(1, 0, 4, 2, 3, 5).reshape(row_count, ATT_HEADS, HEAD_DIM)
    att_normed = rms_scale(attended, attn_out_gain.reshape(ATT_HEADS, HEAD_DIM)).astype(jnp.bfloat16)
    att_normed = att_normed.reshape(row_count, ATT_WIDTH)
    rec_seq = rec_in.reshape(seq_count, length, LRU_WIDTH)
    padded = jnp.pad(rec_seq, ((0, 0), (CONV_TAPS - 1, 0), (0, 0)))
    conv = jnp.zeros((seq_count, length, LRU_WIDTH), jnp.float32)
    for tap in range(CONV_TAPS):
        conv = conv + padded[:, tap:tap + length].astype(jnp.float32) * conv_weight[tap].astype(jnp.float32)
    conv = conv.astype(jnp.bfloat16)
    conv_wide = conv.astype(jnp.float32)
    grouped = conv_wide.reshape(seq_count, length, LRU_BLOCKS, LRU_BLOCK)
    gate_decay = jnp.einsum('bsnd,nde->bsne', grouped, decay_gate_weight.astype(jnp.float32))
    gate_decay = gate_decay.reshape(seq_count, length, LRU_WIDTH)
    gate_input = jnp.einsum('bsnd,nde->bsne', grouped, input_gate_weight.astype(jnp.float32))
    gate_input = gate_input.reshape(seq_count, length, LRU_WIDTH)
    log_decay = -lru_const * jax.nn.sigmoid(gate_decay) * jax.nn.softplus(-decay_param) + decay_extra
    drive = jnp.sqrt(-jnp.expm1(2.0 * log_decay)) * jax.nn.sigmoid(gate_input) * conv_wide
    unused_decay, state = lax.associative_scan(merge_state, (jnp.exp(log_decay), drive), axis=1)
    gated = state * jax.nn.gelu(gate_proj.reshape(seq_count, length, LRU_WIDTH))
    rec_normed = rms_scale(gated.reshape(row_count, LRU_BLOCKS, LRU_BLOCK), rec_out_gain.reshape(LRU_BLOCKS, LRU_BLOCK)).astype(jnp.bfloat16)
    rec_normed = rec_normed.reshape(row_count, LRU_WIDTH)
    mixed = jnp.dot(att_normed, out_att_weight, preferred_element_type=jnp.float32)
    mixed = mixed + jnp.dot(rec_normed, out_rec_weight, preferred_element_type=jnp.float32)
    return mixed.astype(jnp.bfloat16).reshape(seq_count, length, model_width)
```

```python
import functools

import jax
import jax.numpy as jnp
import numpy as np
from jax import lax
from jax.experimental import pallas as pl
from jax.experimental.pallas import tpu as pltpu
from jax.sharding import PartitionSpec as P

D = 2048
LRU_BLOCK = 64
CONV_TAPS = 4


lru_const = 8.0
norm_eps = 1e-06


def from_behind(value, axis, steps):
    count = lax.axis_size(axis)
    leading, last = (max(0, -steps), min(count, count - steps))
    return lax.ppermute(value, axis, [(source, source + steps) for source in range(leading, last)])


def rms_scale(values, gain):
    multiplier = lax.rsqrt(jnp.mean(values * values, axis=-1, keepdims=True) + norm_eps)
    return values * multiplier * gain


def merge_state(earlier, later):
    return (earlier[0] * later[0], later[0] * earlier[1] + later[1])


def block_length(length, span):
    shards = max(length // span, 1)
    group_size = 1
    for trial_size in range(1, shards + 1):
        if shards % trial_size == 0 and trial_size * span <= 1024:
            group_size = trial_size
    sub_size = group_size * span
    if length % sub_size:
        sub_size = length
    return sub_size


def body(
    inputs,
    norm_gain,
    query_weight,
    key_weight,
    value_weight,
    query_gain,
    key_gain,
    forget_cache,
    rec_in_weight,
    rec_gate_weight,
    conv_weight,
    decay_gate_weight,
    input_gate_weight,
    decay_param,
    decay_extra,
    attn_out_gain,
    rec_out_gain,
    out_att_weight,
    out_rec_weight,
):
    seq_count, seq_span, model_width = inputs.shape
    row_count = seq_count * seq_span
    head_dim = query_gain.shape[0]
    att_local = query_weight.shape[1] // head_dim
    kv_local = key_weight.shape[1] // head_dim
    head_group = att_local // kv_local
    channels = rec_in_weight.shape[1]
    normed = rms_scale(
        inputs.reshape(row_count, model_width).astype(jnp.float32), norm_gain
    ).astype(jnp.bfloat16)
    normed_cols = normed.T
    row_contract = (((0,), (0,)), ((), ()))
    kv_cols = key_weight.shape[1]
    pieces = (
        lax.all_gather(query_weight, "sp", axis=0, tiled=True),
        lax.all_gather(key_weight, "sp", axis=0, tiled=True),
        lax.all_gather(value_weight, "sp", axis=0, tiled=True),
        lax.all_gather(rec_in_weight, "sp", axis=0, tiled=True),
        lax.all_gather(rec_gate_weight, "sp", axis=0, tiled=True),
    )
    query_proj, key_proj, value_sum, rec_in_sum, gate_proj = tuple(
        (
            lax.dot_general(
                normed_cols, weight_part, row_contract, preferred_element_type=jnp.float32
            )
            for weight_part in pieces
        )
    )
    queries = rms_scale(query_proj.reshape(row_count, att_local, head_dim), query_gain).astype(
        jnp.bfloat16
    )
    queries = queries.reshape(seq_count, seq_span, kv_local, head_group, head_dim).transpose(
        0, 2, 3, 1, 4
    )
    queries = queries.reshape(seq_count, kv_local, head_group * seq_span, head_dim)
    key_heads = rms_scale(key_proj.reshape(row_count, kv_local, head_dim), key_gain).astype(
        jnp.bfloat16
    )
    key_heads = key_heads.reshape(seq_count, seq_span, kv_cols)
    value_heads = value_sum.astype(jnp.bfloat16).reshape(seq_count, seq_span, kv_cols)
    key_value = jnp.concatenate([key_heads, value_heads], axis=2)
    my_first = lax.axis_index("sp") * seq_span
    own_gates = lax.dynamic_slice_in_dim(forget_cache, my_first, seq_span, 2)
    own_gates = own_gates.reshape(seq_count, kv_local, head_group, seq_span, 1)
    query_pos = my_first + jnp.tile(jnp.arange(seq_span, dtype=jnp.int32), head_group)
    scaling = head_dim ** (-0.5)
    start_state = (
        jnp.full((seq_count, kv_local, head_group * seq_span), -jnp.inf, jnp.float32),
        jnp.zeros((seq_count, kv_local, head_group * seq_span), jnp.float32),
        jnp.zeros((seq_count, kv_local, head_group * seq_span, head_dim), jnp.float32),
    )
    shard_part = lax.all_gather(key_value, "sp", axis=1, tiled=True)
    offset = jnp.int32(0)
    length = shard_part.shape[1]
    sub_size = block_length(length, seq_span)

    def one_step(block_index, carried_state):
        key_first = offset + block_index * sub_size

        def work(carried):
            top_score, totals, accum = carried
            block_rows = lax.dynamic_slice_in_dim(shard_part, block_index * sub_size, sub_size, 1)
            key_block = block_rows[:, :, :kv_cols].reshape(seq_count, sub_size, kv_local, head_dim)
            value_block = block_rows[:, :, kv_cols:].reshape(
                seq_count, sub_size, kv_local, head_dim
            )
            key_gates = lax.dynamic_slice_in_dim(forget_cache, key_first, sub_size, 2)
            key_gates = key_gates.reshape(seq_count, kv_local, head_group, 1, sub_size)
            scores = (
                jnp.einsum(
                    "bhqd,bkhd->bhqk", queries, key_block, preferred_element_type=jnp.float32
                )
                * scaling
            )
            scores = (
                scores.reshape(seq_count, kv_local, head_group, seq_span, sub_size)
                + own_gates
                - key_gates
            )
            scores = scores.reshape(seq_count, kv_local, head_group * seq_span, sub_size)
            visible = (
                query_pos[:, None] >= (key_first + jnp.arange(sub_size, dtype=jnp.int32))[None, :]
            )
            scores = jnp.where(visible, scores, -jnp.inf)
            new_top = jnp.maximum(top_score, jnp.max(scores, axis=-1))
            safe_top = jnp.where(jnp.isfinite(new_top), new_top, 0.0)
            weights = jnp.exp(scores - safe_top[..., None])
            fading = jnp.exp(top_score - safe_top)
            totals = totals * fading + jnp.sum(weights, axis=-1)
            accum = accum * fading[..., None] + jnp.einsum(
                "bhqk,bkhd->bhqd",
                weights.astype(jnp.bfloat16),
                value_block,
                preferred_element_type=jnp.float32,
            )
            return (new_top, totals, accum)

        return lax.cond(
            key_first < my_first + seq_span, work, lambda carried: carried, carried_state
        )

    top_score, totals, accum = lax.fori_loop(0, length // sub_size, one_step, start_state)
    attended = (accum / totals[..., None]).reshape(
        seq_count, kv_local, head_group, seq_span, head_dim
    )
    attended = attended.transpose(0, 3, 1, 2, 4).reshape(row_count, att_local, head_dim)
    att_normed = rms_scale(attended, attn_out_gain.reshape(att_local, head_dim)).astype(
        jnp.bfloat16
    )
    att_normed = att_normed.reshape(row_count, att_local * head_dim)
    rec_in = rec_in_sum.astype(jnp.bfloat16).reshape(seq_count, seq_span, channels)
    before = from_behind(rec_in[:, seq_span - (CONV_TAPS - 1) :, :], "sp", 1)
    extended = jnp.concatenate([before, rec_in], axis=1)
    conv = jnp.zeros((seq_count, seq_span, channels), jnp.float32)
    for tap in range(CONV_TAPS):
        conv = conv + extended[:, tap : tap + seq_span].astype(jnp.float32) * conv_weight[
            tap
        ].astype(jnp.float32)
    conv = conv.astype(jnp.bfloat16)
    blocks_local = decay_gate_weight.shape[0]
    grouped = conv.reshape(seq_count, seq_span, blocks_local, LRU_BLOCK)
    gate_decay = jnp.einsum(
        "bsnd,nde->bsne", grouped, decay_gate_weight, preferred_element_type=jnp.float32
    ).reshape(seq_count, seq_span, channels)
    gate_input = jnp.einsum(
        "bsnd,nde->bsne", grouped, input_gate_weight, preferred_element_type=jnp.float32
    ).reshape(seq_count, seq_span, channels)
    log_decay = (
        -lru_const * jax.nn.sigmoid(gate_decay) * jax.nn.softplus(-decay_param) + decay_extra
    )
    drive = (
        jnp.sqrt(-jnp.expm1(2.0 * log_decay))
        * jax.nn.sigmoid(gate_input)
        * conv.astype(jnp.float32)
    )
    cum_decay, local_state = lax.associative_scan(merge_state, (jnp.exp(log_decay), drive), axis=1)
    every_decay, every_state = (
        lax.all_gather(cum_decay[:, seq_span - 1][None], "sp", axis=0, tiled=True),
        lax.all_gather(local_state[:, seq_span - 1][None], "sp", axis=0, tiled=True),
    )
    prefix_decay, prefix_state = lax.associative_scan(
        merge_state, (every_decay, every_state), axis=0
    )
    position = lax.axis_index("sp")
    earlier_state = lax.dynamic_index_in_dim(
        prefix_state, jnp.maximum(position - 1, 0), 0, keepdims=False
    )
    entering = jnp.where(position > 0, earlier_state, 0.0)
    state = local_state + cum_decay * entering[:, None, :]
    gated = state * jax.nn.gelu(gate_proj.reshape(seq_count, seq_span, channels))
    rec_normed = rms_scale(
        gated.reshape(row_count, blocks_local, LRU_BLOCK),
        rec_out_gain.reshape(blocks_local, LRU_BLOCK),
    ).astype(jnp.bfloat16)
    rec_normed = rec_normed.reshape(row_count, channels)
    out_cols = D // lax.axis_size("tp")
    pieces = row_count * lax.axis_size("tp") // row_count
    terms = jnp.dot(att_normed, out_att_weight, preferred_element_type=jnp.float32) + jnp.dot(
        rec_normed, out_rec_weight, preferred_element_type=jnp.float32
    )
    mixed_cols = lax.psum_scatter(
        terms.reshape(row_count, pieces, out_cols)
        .transpose(1, 0, 2)
        .reshape(pieces * row_count, out_cols)
        .astype(jnp.bfloat16),
        "tp",
        scatter_dimension=0,
        tiled=True,
    )
    return mixed_cols.reshape(seq_count, seq_span, out_cols)


BF16 = jnp.bfloat16
F32 = jnp.float32
HALO = 16
STATE_ROWS = 32


def ring_positions(count):
    return list(range(0, count, 2)) + list(range(count - 1, 0, -2))


def arrival_table(count):
    order = ring_positions(count)
    place = {member: at for at, member in enumerate(order)}
    table = np.zeros((count, count), np.int32)
    for member in range(count):
        at = place[member]
        found = [member]
        for step in range(1, count // 2):
            found += [order[(at - step) % count], order[(at + step) % count]]
        found.append(order[(at + count // 2) % count])
        table[member] = found
    return table


class Ring:
    def __init__(self, own, count, last_forward):
        order = ring_positions(count)
        self.count = count
        self.forward = [(order[at], order[(at + 1) % count]) for at in range(count)]
        self.backward = [(target, source) for source, target in self.forward]
        self.last_forward = last_forward
        self.blocks = [own]
        self.ahead = own
        self.behind = own

    def step(self, number):
        if number < self.count // 2:
            self.ahead = lax.ppermute(self.ahead, "sp", self.forward)
            self.behind = lax.ppermute(self.behind, "sp", self.backward)
            self.blocks += [self.ahead, self.behind]
        elif self.last_forward:
            self.blocks.append(lax.ppermute(self.ahead, "sp", self.forward))
        else:
            self.blocks.append(lax.ppermute(self.behind, "sp", self.backward))


def vmem():
    return pl.BlockSpec(memory_space=pltpu.VMEM)


def smem():
    return pl.BlockSpec(memory_space=pltpu.SMEM)


def call(kernel, outs, operands, scalars=0, scratch=(), name=None, flops=0):
    single = not isinstance(outs, (list, tuple))
    out_shape = outs if single else tuple(outs)
    return pl.pallas_call(
        kernel,
        out_shape=out_shape,
        in_specs=[smem()] * scalars + [vmem()] * (len(operands) - scalars),
        out_specs=vmem() if single else tuple(vmem() for _ in outs),
        scratch_shapes=list(scratch),
        name=name,
        cost_estimate=pl.CostEstimate(flops=flops, bytes_accessed=0, transcendentals=0)
        if flops
        else None,
    )(*operands)


def norm_kernel(rows_ref, halo_ref, gain_ref, out_ref):
    slices, _, width = out_ref.shape
    seq_count, span, _ = rows_ref.shape
    gain = gain_ref[...]
    for seq in range(seq_count):
        first = seq * (HALO + span)
        for values, at, size in ((halo_ref[seq], first, HALO), (rows_ref[seq], first + HALO, span)):
            normed = rms_scale(values.astype(F32), gain).astype(BF16)
            for part in range(slices):
                out_ref[part, at : at + size, :] = normed[:, part * width : (part + 1) * width]


def gathered_dot(index_ref, normed_ref, weight_refs):
    total = None
    for at, weight_ref in enumerate(weight_refs):
        term = jnp.dot(
            normed_ref[index_ref[at]], weight_ref[...], preferred_element_type=F32
        )
        total = term if total is None else total + term
    return total


def minus_expm1(value, exp_value):
    series = jnp.full_like(value, 1.0)
    for term in range(9, 1, -1):
        series = 1.0 + value * (1.0 / term) * series
    return jnp.where(value > -0.5, -value * series, 1.0 - exp_value)


def shifted_down(value, steps, fill):
    moved = pltpu.roll(value, steps, 0)
    row = lax.broadcasted_iota(jnp.int32, value.shape, 0)
    return jnp.where(row >= steps, moved, fill)


def recurrence_kernel(count, head_dim, *refs):
    index_ref, normed_ref = refs[:2]
    weight_refs = refs[2 : 2 + count]
    (
        key_gain_ref,
        taps_ref,
        decay_gate_ref,
        input_gate_ref,
        rate_ref,
        extra_ref,
        message_ref,
        state_ref,
        decay_ref,
        rec_ref,
        ends_ref,
    ) = refs[2 + count :]
    seq_count, span, channels = extra_ref.shape
    kv_width = 2 * head_dim
    sums = gathered_dot(index_ref, normed_ref, weight_refs)
    rec_ref[...] = sums[:, kv_width:].astype(BF16).astype(F32)
    lane = lax.broadcasted_iota(jnp.int32, (span, kv_width), 1)
    ends_ref[...] = jnp.zeros_like(ends_ref)
    halves = channels // kv_width
    for seq in range(seq_count):
        first = seq * (HALO + span)
        rows = pl.ds(seq * span, span)
        kv = sums[first + HALO : first + HALO + span, :kv_width]
        key = jnp.where(lane < head_dim, kv, 0.0)
        mean = jnp.sum(key * key, axis=-1, keepdims=True) * (1.0 / head_dim)
        scaled = kv * lax.rsqrt(mean + norm_eps) * key_gain_ref[...]
        message_ref[rows, :] = jnp.where(lane < head_dim, scaled, kv).astype(BF16)
        conv = jnp.zeros((span, channels), F32)
        for tap in range(CONV_TAPS):
            at = first + HALO - (CONV_TAPS - 1) + tap
            conv = conv + rec_ref[at : at + span, :] * taps_ref[tap : tap + 1, :]
        conv = conv.astype(BF16)
        gate_decay = jnp.dot(conv, decay_gate_ref[...], preferred_element_type=F32)
        gate_input = jnp.dot(conv, input_gate_ref[...], preferred_element_type=F32)
        log_decay = -lru_const * jax.nn.sigmoid(gate_decay) * rate_ref[...] + extra_ref[seq]
        decay = jnp.exp(log_decay)
        state = (
            jnp.sqrt(minus_expm1(2.0 * log_decay, decay * decay))
            * jax.nn.sigmoid(gate_input)
            * conv.astype(F32)
        )
        steps = 1
        while steps < span:
            state = state + decay * shifted_down(state, steps, 0.0)
            decay = decay * shifted_down(decay, steps, 1.0)
            steps *= 2
        state_ref[rows, :] = state
        decay_ref[rows, :] = decay
        for half in range(halves):
            lanes = slice(half * kv_width, (half + 1) * kv_width)
            at = seq * halves + half
            ends_ref[at : at + 1, :] = decay[span - 1 : span, lanes]
            at += seq_count * halves
            ends_ref[at : at + 1, :] = state[span - 1 : span, lanes]
    ends = ends_ref[...]
    high = ends.astype(BF16)
    left = ends - high.astype(F32)
    middle = left.astype(BF16)
    low = (left - middle.astype(F32)).astype(BF16)
    base = seq_count * span
    message_ref[base : base + 16, :] = jnp.concatenate([high, middle], axis=0)
    message_ref[base + 16 : base + 32, :] = jnp.concatenate([low, jnp.zeros_like(low)], axis=0)


def query_kernel(count, head_dim, seq_count, *refs):
    index_ref, normed_ref = refs[:2]
    weight_refs = refs[2 : 2 + count]
    query_gain_ref, query_ref, gelu_ref = refs[2 + count :]
    width = query_ref.shape[2]
    span = query_ref.shape[1]
    heads = query_ref.shape[0] // seq_count
    att = heads * head_dim
    sums = gathered_dot(index_ref, normed_ref, weight_refs)
    lane = lax.broadcasted_iota(jnp.int32, (span, width), 1)
    scaling = head_dim ** (-0.5)
    for seq in range(seq_count):
        first = seq * (HALO + span) + HALO
        rows = sums[first : first + span]
        gelu_ref[seq * span : (seq + 1) * span, :] = jax.nn.gelu(rows[:, att:])
        for head in range(heads):
            pair = rows[:, head // 2 * width : (head // 2 + 1) * width]
            if head % 2:
                pair = pltpu.roll(pair, head_dim, 1)
            own = jnp.where(lane < head_dim, pair, 0.0)
            mean = jnp.sum(own * own, axis=-1, keepdims=True) * (1.0 / head_dim)
            scaled = (own * lax.rsqrt(mean + norm_eps) * query_gain_ref[...]).astype(BF16)
            query_ref[seq * heads + head] = scaled * jnp.asarray(scaling, BF16)


def entering_kernel(count, group, *refs):
    index_ref, place_ref = refs[:2]
    message_refs = refs[2 : 2 + count]
    state_ref, decay_ref, gelu_ref, gain_ref, out_ref, ends_ref = refs[2 + count :]
    rows, channels = state_ref.shape
    width = ends_ref.shape[2]
    halves = channels // width
    seq_count = ends_ref.shape[1] // (2 * halves)
    span = rows // seq_count
    for at, message_ref in enumerate(message_refs):
        parts = message_ref[...].astype(F32)
        ends_ref[index_ref[at]] = parts[0:8] + parts[8:16] + parts[16:24]
    place = place_ref[0]
    half_rows = seq_count * halves
    entering = jnp.zeros((half_rows, width), F32)
    for earlier in range(count - 1):
        ends = ends_ref[earlier]
        merged = ends[:half_rows] * entering + ends[half_rows:]
        entering = jnp.where(earlier < place, merged, entering)
    lane = lax.broadcasted_iota(jnp.int32, (span, width), 1)
    for seq in range(seq_count):
        for half in range(halves):
            lanes = slice(half * width, (half + 1) * width)
            at = seq * halves + half
            part = pl.ds(seq * span, span)
            state = state_ref[part, lanes] + decay_ref[part, lanes] * entering[at : at + 1, :]
            gated = state * gelu_ref[part, lanes]
            square = gated * gated
            total = jnp.sum(square, axis=-1, keepdims=True)
            low = jnp.sum(jnp.where(lane < group, square, 0.0), axis=-1, keepdims=True)
            mean = jnp.where(lane < group, low, total - low) * (1.0 / group)
            out_ref[part, lanes] = (
                gated * lax.rsqrt(mean + norm_eps) * gain_ref[:, lanes]
            ).astype(BF16)


def attention_kernel(count, head_dim, *refs):
    index_ref, place_ref, query_ref = refs[:3]
    message_refs = refs[3 : 3 + count]
    own_gate_ref, key_gate_ref, gain_ref, out_ref, score_ref = refs[3 + count :]
    span, width = query_ref.shape[1:]
    rows = out_ref.shape[0]
    seq_count = rows // span
    heads = query_ref.shape[0] // seq_count
    place = place_ref[0]
    ahead = lax.broadcasted_iota(jnp.int32, (span, span), 1) - lax.broadcasted_iota(
        jnp.int32, (span, span), 0
    )
    lane = lax.broadcasted_iota(jnp.int32, (span, width), 1)
    for seq in range(seq_count):
        keys = pl.ds(seq * span, span)
        queries = query_ref[seq * heads : (seq + 1) * heads].reshape(heads * span, width)
        top = [None] * heads
        for at in range(count):
            block = index_ref[at]
            scores = lax.dot_general(
                queries,
                message_refs[at][keys, :],
                (((1,), (1,)), ((), ())),
                preferred_element_type=F32,
            )
            hidden = ahead > (place - block) * span
            gates = key_gate_ref[block]
            for head in range(heads):
                line = seq * heads + head
                score = scores[head * span : (head + 1) * span]
                score = score + own_gate_ref[line] - gates[line : line + 1, :]
                score = jnp.where(hidden, -jnp.inf, score)
                score_ref[at, head * span : (head + 1) * span, :] = score
                top[head] = score if at == 0 else jnp.maximum(top[head], score)
        top = [jnp.max(part, axis=-1, keepdims=True) for part in top]
        totals = [None] * heads
        weighted = None
        for at in range(count):
            weights = []
            for head in range(heads):
                part = jnp.exp(score_ref[at, head * span : (head + 1) * span, :] - top[head])
                totals[head] = part if at == 0 else totals[head] + part
                weights.append(part.astype(BF16))
            term = jnp.dot(
                jnp.concatenate(weights, axis=0),
                message_refs[at][keys, :],
                preferred_element_type=F32,
            )
            weighted = term if at == 0 else weighted + term
        outs = []
        for head in range(heads):
            total = jnp.sum(totals[head], axis=-1, keepdims=True)
            attended = weighted[head * span : (head + 1) * span] / total
            attended = jnp.where(lane >= head_dim, attended, 0.0)
            mean = jnp.sum(attended * attended, axis=-1, keepdims=True) * (1.0 / head_dim)
            outs.append(attended * lax.rsqrt(mean + norm_eps))
        for pair in range(heads // 2):
            lanes = slice(pair * width, (pair + 1) * width)
            joined = jnp.where(
                lane < head_dim, pltpu.roll(outs[2 * pair], head_dim, 1), outs[2 * pair + 1]
            )
            out_ref[keys, lanes] = (joined * gain_ref[:, lanes]).astype(BF16)


def output_kernel(pieces, has_base, *refs):
    left_refs = refs[:pieces]
    right_refs = refs[pieces : 2 * pieces]
    out_ref = refs[-1]
    total = refs[2 * pieces][...] if has_base else None
    for left_ref, right_ref in zip(left_refs, right_refs):
        term = jnp.dot(left_ref[...], right_ref[...], preferred_element_type=F32)
        total = term if total is None else total + term
    out_ref[...] = total.astype(out_ref.dtype)


def tp_spread(value, count):
    found = {0: value}
    bit = count // 2
    while bit:
        members = sorted(found)
        pairs = [(source, source ^ bit) for source in range(count)]
        moved = lax.ppermute(jnp.stack([found[member] for member in members]), "tp", pairs)
        for at, member in enumerate(members):
            found[member ^ bit] = moved[at]
        bit //= 2
    return [found[member] for member in range(count)]


def ring_body(
    inputs,
    norm_gain,
    query_weight,
    key_weight,
    value_weight,
    query_gain,
    key_gain,
    forget_cache,
    rec_in_weight,
    rec_gate_weight,
    conv_weight,
    decay_gate_weight,
    input_gate_weight,
    decay_param,
    decay_extra,
    attn_out_gain,
    rec_out_gain,
    out_att_weight,
    out_rec_weight,
):
    count = lax.axis_size("sp")
    tp_count = lax.axis_size("tp")
    place = lax.axis_index("sp")
    tp_place = lax.axis_index("tp")
    seq_count, span, model_width = inputs.shape
    rows = seq_count * span
    head_dim = query_gain.shape[0]
    width = 2 * head_dim
    att_width = query_weight.shape[1]
    heads = att_width // head_dim
    channels = rec_in_weight.shape[1]
    ext_rows = seq_count * (HALO + span)
    index = lax.dynamic_index_in_dim(jnp.asarray(arrival_table(count)), place, 0, keepdims=False)
    place_row = place.reshape(1).astype(jnp.int32)

    first_ring = Ring(
        jnp.concatenate([key_weight, value_weight, rec_in_weight], axis=1), count, True
    )
    second_ring = Ring(jnp.concatenate([query_weight, rec_gate_weight], axis=1), count, False)
    first_ring.step(1)
    second_ring.step(1)

    shift = [(member, (member + 1) % count) for member in range(count)]
    halo = lax.ppermute(inputs[:, span - (CONV_TAPS - 1) :, :], "sp", shift)
    halo = jnp.where(place > 0, halo, jnp.zeros_like(halo))
    halo = jnp.pad(halo, ((0, 0), (HALO - (CONV_TAPS - 1), 0), (0, 0)))
    normed = call(
        norm_kernel,
        jax.ShapeDtypeStruct((count, ext_rows, model_width // count), BF16),
        [inputs, halo, norm_gain.reshape(1, model_width)],
        name="norm",
    )
    out_cols = model_width // tp_count
    out_weight = [
        lax.dynamic_slice_in_dim(
            jnp.concatenate([out_att_weight, out_rec_weight], axis=0),
            (tp_place ^ member) * out_cols,
            out_cols,
            1,
        )
        for member in range(tp_count)
    ]
    for member in range(1, tp_count):
        pairs = [(source, source ^ member) for source in range(tp_count)]
        out_weight[member] = lax.ppermute(out_weight[member], "tp", pairs)

    for number in range(2, count // 2 + 1):
        first_ring.step(number)
        second_ring.step(number)

    blocks = decay_gate_weight.shape[0]

    def block_diagonal(weight):
        tiled = jnp.tile(weight.reshape(channels, LRU_BLOCK), (1, blocks))
        group = jnp.arange(channels, dtype=jnp.int32) // LRU_BLOCK
        return jnp.where(group[:, None] == group[None, :], tiled, jnp.zeros_like(tiled))

    key_gain_row = jnp.concatenate([key_gain, jnp.ones_like(key_gain)]).reshape(1, width)
    message, local_state, cum_decay = call(
        functools.partial(recurrence_kernel, count, head_dim),
        [
            jax.ShapeDtypeStruct((rows + STATE_ROWS, width), BF16),
            jax.ShapeDtypeStruct((rows, channels), F32),
            jax.ShapeDtypeStruct((rows, channels), F32),
        ],
        [
            index,
            normed,
            *first_ring.blocks,
            key_gain_row,
            conv_weight.astype(F32),
            block_diagonal(decay_gate_weight),
            block_diagonal(input_gate_weight),
            jax.nn.softplus(-decay_param).reshape(1, channels),
            decay_extra,
        ],
        scalars=1,
        scratch=[pltpu.VMEM((ext_rows, channels), F32), pltpu.VMEM((8, width), F32)],
        name="recurrence",
    )
    message_ring = Ring(message, count, True)
    for number in range(1, count // 2 + 1):
        message_ring.step(number)

    query_gain_row = jnp.concatenate([query_gain, jnp.zeros_like(query_gain)]).reshape(1, width)
    queries, gelu = call(
        functools.partial(query_kernel, count, head_dim, seq_count),
        [
            jax.ShapeDtypeStruct((seq_count * heads, span, width), BF16),
            jax.ShapeDtypeStruct((rows, channels), F32),
        ],
        [index, normed, *second_ring.blocks, query_gain_row],
        scalars=1,
        name="query",
    )
    messages = message_ring.blocks
    rec_normed = call(
        functools.partial(entering_kernel, count, LRU_BLOCK),
        jax.ShapeDtypeStruct((rows, channels), BF16),
        [
            index,
            place_row,
            *[part[rows:] for part in messages],
            local_state,
            cum_decay,
            gelu,
            rec_out_gain.reshape(1, channels),
        ],
        scalars=2,
        scratch=[pltpu.VMEM((count, 8, width), F32)],
        name="entering",
    )
    gates = forget_cache.reshape(seq_count * heads, count, span)
    own_gates = lax.dynamic_index_in_dim(gates, place, 1, keepdims=False)
    att_normed = call(
        functools.partial(attention_kernel, count, head_dim),
        jax.ShapeDtypeStruct((rows, att_width), BF16),
        [
            index,
            place_row,
            queries,
            *messages,
            own_gates[:, :, None],
            gates.transpose(1, 0, 2),
            attn_out_gain.reshape(1, att_width),
        ],
        scalars=2,
        scratch=[pltpu.VMEM((count, heads * span, span), F32)],
        name="attention",
    )
    rec_parts = tp_spread(rec_normed, tp_count)
    att_parts = tp_spread(att_normed, tp_count)
    from_rec = call(
        functools.partial(output_kernel, tp_count, False),
        jax.ShapeDtypeStruct((rows, out_cols), F32),
        [*rec_parts, *[part[att_width:] for part in out_weight]],
        name="from_rec",
    )
    mixed = call(
        functools.partial(output_kernel, tp_count, True),
        jax.ShapeDtypeStruct((rows, out_cols), BF16),
        [*att_parts, *[part[:att_width] for part in out_weight], from_rec],
        name="mixed",
    )
    return mixed.reshape(seq_count, span, out_cols)


def solution(mesh):
    count, tp_count = mesh.shape["sp"], mesh.shape["tp"]
    short = 4 <= count <= 16 and count % 2 == 0 and tp_count & (tp_count - 1) == 0
    return jax.shard_map(
        ring_body if short else body,
        mesh=mesh,
        in_specs=(
            P(None, "sp", None),
            P(),
            P("sp", "tp"),
            P("sp", "tp"),
            P("sp", "tp"),
            P(),
            P(),
            P(None, "tp", None),
            P("sp", "tp"),
            P("sp", "tp"),
            P(None, "tp"),
            P("tp", None, None),
            P("tp", None, None),
            P("tp"),
            P(None, "sp", "tp"),
            P("tp"),
            P("tp"),
            P("tp", None),
            P("tp", None),
        ),
        out_specs=P(None, "sp", "tp"),
        check_vma=False,
    )
```

```python
import functools

import jax
import jax.numpy as jnp
from jax import lax
from jax.experimental import pallas as pl
from jax.experimental.pallas import tpu as pltpu
from jax.sharding import PartitionSpec as P

D = 2048
LRU_BLOCK = 64
CONV_TAPS = 4


lru_const = 8.0
norm_eps = 1e-06


def from_behind(value, axis, steps):
    count = lax.axis_size(axis)
    leading, last = (max(0, -steps), min(count, count - steps))
    return lax.ppermute(value, axis, [(source, source + steps) for source in range(leading, last)])


def rms_scale(values, gain):
    multiplier = lax.rsqrt(jnp.mean(values * values, axis=-1, keepdims=True) + norm_eps)
    return values * multiplier * gain


def merge_state(earlier, later):
    return (earlier[0] * later[0], later[0] * earlier[1] + later[1])


def block_length(length, span):
    shards = max(length // span, 1)
    group_size = 1
    for trial_size in range(1, shards + 1):
        if shards % trial_size == 0 and trial_size * span <= 1024:
            group_size = trial_size
    sub_size = group_size * span
    if length % sub_size:
        sub_size = length
    return sub_size


def body(
    inputs,
    norm_gain,
    query_weight,
    key_weight,
    value_weight,
    query_gain,
    key_gain,
    forget_cache,
    rec_in_weight,
    rec_gate_weight,
    conv_weight,
    decay_gate_weight,
    input_gate_weight,
    decay_param,
    decay_extra,
    attn_out_gain,
    rec_out_gain,
    out_att_weight,
    out_rec_weight,
):
    seq_count, seq_span, model_width = inputs.shape
    row_count = seq_count * seq_span
    head_dim = query_gain.shape[0]
    att_local = query_weight.shape[1] // head_dim
    kv_local = key_weight.shape[1] // head_dim
    head_group = att_local // kv_local
    channels = rec_in_weight.shape[1]
    normed = rms_scale(
        inputs.reshape(row_count, model_width).astype(jnp.float32), norm_gain
    ).astype(jnp.bfloat16)
    normed_cols = normed.T
    row_contract = (((0,), (0,)), ((), ()))
    kv_cols = key_weight.shape[1]
    pieces = (
        lax.all_gather(query_weight, "sp", axis=0, tiled=True),
        lax.all_gather(key_weight, "sp", axis=0, tiled=True),
        lax.all_gather(value_weight, "sp", axis=0, tiled=True),
        lax.all_gather(rec_in_weight, "sp", axis=0, tiled=True),
        lax.all_gather(rec_gate_weight, "sp", axis=0, tiled=True),
    )
    query_proj, key_proj, value_sum, rec_in_sum, gate_proj = tuple(
        (
            lax.dot_general(
                normed_cols, weight_part, row_contract, preferred_element_type=jnp.float32
            )
            for weight_part in pieces
        )
    )
    queries = rms_scale(query_proj.reshape(row_count, att_local, head_dim), query_gain).astype(
        jnp.bfloat16
    )
    queries = queries.reshape(seq_count, seq_span, kv_local, head_group, head_dim).transpose(
        0, 2, 3, 1, 4
    )
    queries = queries.reshape(seq_count, kv_local, head_group * seq_span, head_dim)
    key_heads = rms_scale(key_proj.reshape(row_count, kv_local, head_dim), key_gain).astype(
        jnp.bfloat16
    )
    key_heads = key_heads.reshape(seq_count, seq_span, kv_cols)
    value_heads = value_sum.astype(jnp.bfloat16).reshape(seq_count, seq_span, kv_cols)
    key_value = jnp.concatenate([key_heads, value_heads], axis=2)
    my_first = lax.axis_index("sp") * seq_span
    own_gates = lax.dynamic_slice_in_dim(forget_cache, my_first, seq_span, 2)
    own_gates = own_gates.reshape(seq_count, kv_local, head_group, seq_span, 1)
    query_pos = my_first + jnp.tile(jnp.arange(seq_span, dtype=jnp.int32), head_group)
    scaling = head_dim ** (-0.5)
    start_state = (
        jnp.full((seq_count, kv_local, head_group * seq_span), -jnp.inf, jnp.float32),
        jnp.zeros((seq_count, kv_local, head_group * seq_span), jnp.float32),
        jnp.zeros((seq_count, kv_local, head_group * seq_span, head_dim), jnp.float32),
    )
    shard_part = lax.all_gather(key_value, "sp", axis=1, tiled=True)
    offset = jnp.int32(0)
    length = shard_part.shape[1]
    sub_size = block_length(length, seq_span)

    def one_step(block_index, carried_state):
        key_first = offset + block_index * sub_size

        def work(carried):
            top_score, totals, accum = carried
            block_rows = lax.dynamic_slice_in_dim(shard_part, block_index * sub_size, sub_size, 1)
            key_block = block_rows[:, :, :kv_cols].reshape(seq_count, sub_size, kv_local, head_dim)
            value_block = block_rows[:, :, kv_cols:].reshape(
                seq_count, sub_size, kv_local, head_dim
            )
            key_gates = lax.dynamic_slice_in_dim(forget_cache, key_first, sub_size, 2)
            key_gates = key_gates.reshape(seq_count, kv_local, head_group, 1, sub_size)
            scores = (
                jnp.einsum(
                    "bhqd,bkhd->bhqk", queries, key_block, preferred_element_type=jnp.float32
                )
                * scaling
            )
            scores = (
                scores.reshape(seq_count, kv_local, head_group, seq_span, sub_size)
                + own_gates
                - key_gates
            )
            scores = scores.reshape(seq_count, kv_local, head_group * seq_span, sub_size)
            visible = (
                query_pos[:, None] >= (key_first + jnp.arange(sub_size, dtype=jnp.int32))[None, :]
            )
            scores = jnp.where(visible, scores, -jnp.inf)
            new_top = jnp.maximum(top_score, jnp.max(scores, axis=-1))
            safe_top = jnp.where(jnp.isfinite(new_top), new_top, 0.0)
            weights = jnp.exp(scores - safe_top[..., None])
            fading = jnp.exp(top_score - safe_top)
            totals = totals * fading + jnp.sum(weights, axis=-1)
            accum = accum * fading[..., None] + jnp.einsum(
                "bhqk,bkhd->bhqd",
                weights.astype(jnp.bfloat16),
                value_block,
                preferred_element_type=jnp.float32,
            )
            return (new_top, totals, accum)

        return lax.cond(
            key_first < my_first + seq_span, work, lambda carried: carried, carried_state
        )

    _, totals, accum = lax.fori_loop(0, length // sub_size, one_step, start_state)
    attended = (accum / totals[..., None]).reshape(
        seq_count, kv_local, head_group, seq_span, head_dim
    )
    attended = attended.transpose(0, 3, 1, 2, 4).reshape(row_count, att_local, head_dim)
    att_normed = rms_scale(attended, attn_out_gain.reshape(att_local, head_dim)).astype(
        jnp.bfloat16
    )
    att_normed = att_normed.reshape(row_count, att_local * head_dim)
    rec_in = rec_in_sum.astype(jnp.bfloat16).reshape(seq_count, seq_span, channels)
    before = from_behind(rec_in[:, seq_span - (CONV_TAPS - 1) :, :], "sp", 1)
    extended = jnp.concatenate([before, rec_in], axis=1)
    conv = jnp.zeros((seq_count, seq_span, channels), jnp.float32)
    for tap in range(CONV_TAPS):
        conv = conv + extended[:, tap : tap + seq_span].astype(jnp.float32) * conv_weight[
            tap
        ].astype(jnp.float32)
    conv = conv.astype(jnp.bfloat16)
    blocks_local = decay_gate_weight.shape[0]
    grouped = conv.reshape(seq_count, seq_span, blocks_local, LRU_BLOCK)
    gate_decay = jnp.einsum(
        "bsnd,nde->bsne", grouped, decay_gate_weight, preferred_element_type=jnp.float32
    ).reshape(seq_count, seq_span, channels)
    gate_input = jnp.einsum(
        "bsnd,nde->bsne", grouped, input_gate_weight, preferred_element_type=jnp.float32
    ).reshape(seq_count, seq_span, channels)
    log_decay = (
        -lru_const * jax.nn.sigmoid(gate_decay) * jax.nn.softplus(-decay_param) + decay_extra
    )
    drive = (
        jnp.sqrt(-jnp.expm1(2.0 * log_decay))
        * jax.nn.sigmoid(gate_input)
        * conv.astype(jnp.float32)
    )
    cum_decay, local_state = lax.associative_scan(merge_state, (jnp.exp(log_decay), drive), axis=1)
    every_decay, every_state = (
        lax.all_gather(cum_decay[:, seq_span - 1][None], "sp", axis=0, tiled=True),
        lax.all_gather(local_state[:, seq_span - 1][None], "sp", axis=0, tiled=True),
    )
    _, prefix_state = lax.associative_scan(merge_state, (every_decay, every_state), axis=0)
    position = lax.axis_index("sp")
    earlier_state = lax.dynamic_index_in_dim(
        prefix_state, jnp.maximum(position - 1, 0), 0, keepdims=False
    )
    entering = jnp.where(position > 0, earlier_state, 0.0)
    state = local_state + cum_decay * entering[:, None, :]
    gated = state * jax.nn.gelu(gate_proj.reshape(seq_count, seq_span, channels))
    rec_normed = rms_scale(
        gated.reshape(row_count, blocks_local, LRU_BLOCK),
        rec_out_gain.reshape(blocks_local, LRU_BLOCK),
    ).astype(jnp.bfloat16)
    rec_normed = rec_normed.reshape(row_count, channels)
    out_cols = D // lax.axis_size("tp")
    pieces = row_count * lax.axis_size("tp") // row_count
    terms = jnp.dot(att_normed, out_att_weight, preferred_element_type=jnp.float32) + jnp.dot(
        rec_normed, out_rec_weight, preferred_element_type=jnp.float32
    )
    mixed_cols = lax.psum_scatter(
        terms.reshape(row_count, pieces, out_cols)
        .transpose(1, 0, 2)
        .reshape(pieces * row_count, out_cols)
        .astype(jnp.bfloat16),
        "tp",
        scatter_dimension=0,
        tiled=True,
    )
    return mixed_cols.reshape(seq_count, seq_span, out_cols)


BF16 = jnp.bfloat16
F32 = jnp.float32
HALO = 16
STATE_ROWS = 32
KERNEL_VMEM = 10 << 20


def ring_positions(count):
    return list(range(0, count, 2)) + list(range(count - 1, 0, -2))


def arrivals(place, count):
    at = jnp.where(place % 2 == 0, place // 2, count - 1 - place // 2)

    def member(position):
        position = (position + count) % count
        return jnp.where(position < count // 2, 2 * position, 2 * (count - 1 - position) + 1)

    found = [place]
    for step in range(1, count // 2):
        found += [member(at - step), member(at + step)]
    return found + [member(at + count // 2)]


class Ring:
    def __init__(self, own, count, last_forward):
        order = ring_positions(count)
        self.count = count
        self.forward = [(order[at], order[(at + 1) % count]) for at in range(count)]
        self.backward = [(target, source) for source, target in self.forward]
        self.last_forward = last_forward
        self.blocks = [own]
        self.ahead = own
        self.behind = own

    def step(self, number):
        last = number == self.count // 2
        if not last or self.last_forward:
            self.ahead = lax.ppermute(self.ahead, "sp", self.forward)
            self.blocks.append(self.ahead)
        if not last or not self.last_forward:
            self.behind = lax.ppermute(self.behind, "sp", self.backward)
            self.blocks.append(self.behind)


def vmem():
    return pl.BlockSpec(memory_space=pltpu.VMEM)


def call(kernel, outs, operands, scratch=()):
    single = not isinstance(outs, (list, tuple))
    return pl.pallas_call(
        kernel,
        out_shape=outs if single else tuple(outs),
        in_specs=[vmem()] * len(operands),
        out_specs=vmem() if single else tuple(vmem() for _ in outs),
        scratch_shapes=list(scratch),
        compiler_params=pltpu.CompilerParams(vmem_limit_bytes=KERNEL_VMEM),
    )(*operands)


def pack_kernel(key_ref, value_ref, rec_ref, out_ref):
    at = 0
    for part_ref in (key_ref, value_ref):
        size = part_ref.shape[0]
        out_ref[:, at : at + size] = part_ref[...].astype(F32).T.astype(BF16)
        at += size
    out_ref[:, at:] = rec_ref[...]


def pack_out_kernel(att_ref, rec_ref, *out_refs):
    place = lax.axis_index("tp")
    rows = att_ref.shape[0]
    for member, out_ref in enumerate(out_refs):
        width = out_ref.shape[1]
        columns = pl.ds(pl.multiple_of((place ^ member) * width, width), width)
        out_ref[:rows, :] = att_ref[:, columns]
        out_ref[rows:, :] = rec_ref[:, columns]


def block_diagonal(weight_ref):
    blocks, size, _ = weight_ref.shape
    tall = weight_ref[...].reshape(blocks * size, size)
    tiled = jnp.concatenate([tall] * blocks, axis=1)
    row = lax.broadcasted_iota(jnp.int32, tiled.shape, 0) // size
    column = lax.broadcasted_iota(jnp.int32, tiled.shape, 1) // size
    return jnp.where(row == column, tiled, jnp.zeros_like(tiled))


def norm_kernel(rows_ref, halo_ref, gain_ref, decay_ref, input_ref, out_ref, gates_ref):
    slices, _, width = out_ref.shape
    seq_count, span, _ = rows_ref.shape
    gain = gain_ref[...]
    kept = jnp.where(lax.axis_index("sp") > 0, 1.0, 0.0)
    for seq in range(seq_count):
        first = seq * (HALO + span)
        tail = halo_ref[seq].astype(F32) * kept
        tail = jnp.concatenate([jnp.zeros_like(tail), tail], axis=0)
        body_rows = rows_ref[seq].astype(F32)
        for values, at, size in ((tail, first, HALO), (body_rows, first + HALO, span)):
            normed = rms_scale(values, gain).astype(BF16)
            for part in range(slices):
                out_ref[part, at : at + size, :] = normed[:, part * width : (part + 1) * width]
    channels = gates_ref.shape[0]
    gates_ref[:, :channels] = block_diagonal(decay_ref)
    gates_ref[:, channels:] = block_diagonal(input_ref)


def softplus(value):
    small = jnp.exp(-jnp.abs(value))
    series = jnp.full_like(small, 1.0 / 7)
    for term in range(6, 0, -1):
        series = 1.0 / term - small * series
    return jnp.maximum(value, 0.0) + jnp.where(
        small < 0.05, small * series, jnp.log(1.0 + small)
    )


def gathered_dot(normed_ref, weight_refs, count, first=0, total=None):
    found = arrivals(lax.axis_index("sp"), count)[first:]
    for index, weight_ref in zip(found, weight_refs):
        term = jnp.dot(normed_ref[index], weight_ref[...], preferred_element_type=F32)
        total = term if total is None else total + term
    return total


def part_kernel(count, normed_ref, *refs):
    refs[-1][...] = gathered_dot(normed_ref, refs[:-1], count)


def minus_expm1(value, exp_value):
    series = jnp.full_like(value, 1.0)
    for term in range(9, 1, -1):
        series = 1.0 + value * (1.0 / term) * series
    return jnp.where(value > -0.5, -value * series, 1.0 - exp_value)


def shifted_down(value, steps, fill):
    moved = pltpu.roll(value, steps, 0)
    row = lax.broadcasted_iota(jnp.int32, value.shape, 0)
    return jnp.where(row >= steps, moved, fill)


def recurrence_kernel(count, head_dim, *refs):
    (
        normed_ref,
        part_ref,
        last_ref,
        key_gain_ref,
        taps_ref,
        gates_ref,
        decay_param_ref,
        extra_ref,
        message_ref,
        state_ref,
        decay_ref,
        rec_ref,
        ends_ref,
    ) = refs
    seq_count, span, channels = extra_ref.shape
    kv_width = 2 * head_dim
    sums = gathered_dot(normed_ref, [last_ref], count, count - 1, part_ref[...])
    rec_ref[...] = sums[:, kv_width:].astype(BF16).astype(F32)
    rate = softplus(-decay_param_ref[...])
    taps = taps_ref[...].astype(F32)
    key_gain = jnp.concatenate([key_gain_ref[...]] * 2, axis=1)
    lane = lax.broadcasted_iota(jnp.int32, (span, kv_width), 1)
    ends_ref[...] = jnp.zeros_like(ends_ref)
    halves = channels // kv_width
    for seq in range(seq_count):
        first = seq * (HALO + span)
        rows = pl.ds(seq * span, span)
        kv = sums[first + HALO : first + HALO + span, :kv_width]
        key = jnp.where(lane < head_dim, kv, 0.0)
        mean = jnp.sum(key * key, axis=-1, keepdims=True) * (1.0 / head_dim)
        scaled = kv * lax.rsqrt(mean + norm_eps) * key_gain
        message_ref[rows, :] = jnp.where(lane < head_dim, scaled, kv).astype(BF16)
        conv = jnp.zeros((span, channels), F32)
        for tap in range(CONV_TAPS):
            at = first + HALO - (CONV_TAPS - 1) + tap
            conv = conv + rec_ref[at : at + span, :] * taps[tap : tap + 1, :]
        conv = conv.astype(BF16)
        gated = jnp.dot(conv, gates_ref[...], preferred_element_type=F32)
        gate_decay, gate_input = gated[:, :channels], gated[:, channels:]
        log_decay = -lru_const * jax.nn.sigmoid(gate_decay) * rate + extra_ref[seq]
        decay = jnp.exp(log_decay)
        state = (
            jnp.sqrt(minus_expm1(2.0 * log_decay, decay * decay))
            * jax.nn.sigmoid(gate_input)
            * conv.astype(F32)
        )
        steps = 1
        while steps < span:
            state = state + decay * shifted_down(state, steps, 0.0)
            decay = decay * shifted_down(decay, steps, 1.0)
            steps *= 2
        state_ref[rows, :] = state
        decay_ref[rows, :] = decay
        for half in range(halves):
            lanes = slice(half * kv_width, (half + 1) * kv_width)
            at = seq * halves + half
            ends_ref[at : at + 1, :] = decay[span - 1 : span, lanes]
            at += seq_count * halves
            ends_ref[at : at + 1, :] = state[span - 1 : span, lanes]
    ends = ends_ref[...]
    high = ends.astype(BF16)
    left = ends - high.astype(F32)
    middle = left.astype(BF16)
    low = (left - middle.astype(F32)).astype(BF16)
    base = seq_count * span
    message_ref[base : base + 16, :] = jnp.concatenate([high, middle], axis=0)
    message_ref[base + 16 : base + 32, :] = jnp.concatenate([low, jnp.zeros_like(low)], axis=0)


def query_kernel(count, head_dim, seq_count, normed_ref, *refs):
    query_gain_ref, query_ref = refs[-2:]
    width = query_ref.shape[2]
    span = query_ref.shape[1]
    heads = query_ref.shape[0] // seq_count
    gain = jnp.concatenate([query_gain_ref[...]] * 2, axis=1)
    sums = gathered_dot(normed_ref, refs[:-2], count)
    lane = lax.broadcasted_iota(jnp.int32, (span, width), 1)
    scaling = head_dim ** (-0.5)
    for seq in range(seq_count):
        first = seq * (HALO + span) + HALO
        rows = sums[first : first + span]
        for head in range(heads):
            pair = rows[:, head // 2 * width : (head // 2 + 1) * width]
            if head % 2:
                pair = pltpu.roll(pair, head_dim, 1)
            own = jnp.where(lane < head_dim, pair, 0.0)
            mean = jnp.sum(own * own, axis=-1, keepdims=True) * (1.0 / head_dim)
            scaled = (own * lax.rsqrt(mean + norm_eps) * gain).astype(BF16)
            query_ref[seq * heads + head] = scaled * jnp.asarray(scaling, BF16)


def entering_kernel(count, group, *refs):
    place = lax.axis_index("sp")
    message_refs = refs[:count]
    (
        state_ref,
        decay_ref,
        normed_ref,
        part_ref,
        last_ref,
        gain_ref,
        out_ref,
        ends_ref,
    ) = refs[count:]
    gate = gathered_dot(normed_ref, [last_ref], count, count - 1, part_ref[...])
    rows, channels = state_ref.shape
    width = ends_ref.shape[2]
    halves = channels // width
    seq_count = ends_ref.shape[1] // (2 * halves)
    span = rows // seq_count
    for index, message_ref in zip(arrivals(place, count), message_refs):
        parts = message_ref[rows:, :].astype(F32)
        ends_ref[index] = parts[0:8] + parts[8:16] + parts[16:24]
    half_rows = seq_count * halves
    entering = jnp.zeros((half_rows, width), F32)
    for earlier in range(count - 1):
        ends = ends_ref[earlier]
        merged = ends[:half_rows] * entering + ends[half_rows:]
        entering = jnp.where(earlier < place, merged, entering)
    lane = lax.broadcasted_iota(jnp.int32, (span, width), 1)
    for seq in range(seq_count):
        for half in range(halves):
            lanes = slice(half * width, (half + 1) * width)
            at = seq * halves + half
            part = pl.ds(seq * span, span)
            first = seq * (HALO + span) + HALO
            state = state_ref[part, lanes] + decay_ref[part, lanes] * entering[at : at + 1, :]
            gated = state * jax.nn.gelu(gate[first : first + span, lanes])
            square = gated * gated
            total = jnp.sum(square, axis=-1, keepdims=True)
            low = jnp.sum(jnp.where(lane < group, square, 0.0), axis=-1, keepdims=True)
            mean = jnp.where(lane < group, low, total - low) * (1.0 / group)
            out_ref[part, lanes] = (
                gated * lax.rsqrt(mean + norm_eps) * gain_ref[:, lanes]
            ).astype(BF16)


def attention_kernel(count, head_dim, *refs):
    query_ref = refs[0]
    message_refs = refs[1 : 1 + count]
    gate_ref, gain_ref, out_ref, score_ref = refs[1 + count :]
    span, width = query_ref.shape[1:]
    rows = out_ref.shape[0]
    seq_count = rows // span
    heads = query_ref.shape[0] // seq_count
    place = lax.axis_index("sp")
    found = arrivals(place, count)
    ahead = lax.broadcasted_iota(jnp.int32, (span, span), 1) - lax.broadcasted_iota(
        jnp.int32, (span, span), 0
    )
    lane = lax.broadcasted_iota(jnp.int32, (span, width), 1)
    for seq in range(seq_count):
        keys = pl.ds(seq * span, span)
        queries = query_ref[seq * heads : (seq + 1) * heads].reshape(heads * span, width)
        top = [None] * heads
        own = gate_ref[seq, :, pl.ds(pl.multiple_of(place * span, span), span)]
        own = jnp.concatenate([own, jnp.zeros((span - heads, span), F32)], axis=0).T
        for at, block in enumerate(found):
            scores = lax.dot_general(
                queries,
                message_refs[at][keys, :],
                (((1,), (1,)), ((), ())),
                preferred_element_type=F32,
            )
            hidden = ahead > (place - block) * span
            gates = gate_ref[seq, :, pl.ds(pl.multiple_of(block * span, span), span)]
            for head in range(heads):
                score = scores[head * span : (head + 1) * span]
                score = score + own[:, head : head + 1] - gates[head : head + 1, :]
                score = jnp.where(hidden, -jnp.inf, score)
                score_ref[at, head * span : (head + 1) * span, :] = score
                top[head] = score if at == 0 else jnp.maximum(top[head], score)
        top = [jnp.max(part, axis=-1, keepdims=True) for part in top]
        totals = [None] * heads
        weighted = None
        for at in range(count):
            weights = []
            for head in range(heads):
                part = jnp.exp(score_ref[at, head * span : (head + 1) * span, :] - top[head])
                totals[head] = part if at == 0 else totals[head] + part
                weights.append(part.astype(BF16))
            term = jnp.dot(
                jnp.concatenate(weights, axis=0),
                message_refs[at][keys, :],
                preferred_element_type=F32,
            )
            weighted = term if at == 0 else weighted + term
        outs = []
        for head in range(heads):
            total = jnp.sum(totals[head], axis=-1, keepdims=True)
            attended = weighted[head * span : (head + 1) * span] / total
            attended = jnp.where(lane >= head_dim, attended, 0.0)
            mean = jnp.sum(attended * attended, axis=-1, keepdims=True) * (1.0 / head_dim)
            outs.append(attended * lax.rsqrt(mean + norm_eps))
        for pair in range(heads // 2):
            lanes = slice(pair * width, (pair + 1) * width)
            joined = jnp.where(
                lane < head_dim, pltpu.roll(outs[2 * pair], head_dim, 1), outs[2 * pair + 1]
            )
            out_ref[keys, lanes] = (joined * gain_ref[:, lanes]).astype(BF16)


def output_kernel(uses, has_base, *refs):
    out_ref = refs[-1]
    total = refs[-2][...] if has_base else None
    for left, right, half in uses:
        rows = refs[left].shape[1]
        term = jnp.dot(
            refs[left][...],
            refs[right][half * rows : (half + 1) * rows, :],
            preferred_element_type=F32,
        )
        total = term if total is None else total + term
    out_ref[...] = total.astype(out_ref.dtype)


def tp_spread(value, count):
    bits = [1 << at for at in range(count.bit_length() - 1)]
    found = {0: value}
    for bit in reversed(bits):
        pairs = [(source, source ^ bit) for source in range(count)]
        for member in sorted(found):
            found[member ^ bit] = lax.ppermute(found[member], "tp", pairs)
    return [found[member] for member in range(count)]


def ring_body(
    inputs,
    norm_gain,
    query_weight,
    key_weight,
    value_weight,
    query_gain,
    key_gain,
    forget_cache,
    rec_in_weight,
    rec_gate_weight,
    conv_weight,
    decay_gate_weight,
    input_gate_weight,
    decay_param,
    decay_extra,
    attn_out_gain,
    rec_out_gain,
    out_att_weight,
    out_rec_weight,
):
    count = lax.axis_size("sp")
    tp_count = lax.axis_size("tp")
    seq_count, span, model_width = inputs.shape
    rows = seq_count * span
    head_dim = query_gain.shape[0]
    width = 2 * head_dim
    att_width = query_weight.shape[1]
    heads = att_width // head_dim
    channels = rec_in_weight.shape[1]
    ext_rows = seq_count * (HALO + span)
    out_cols = model_width // tp_count
    query_ring = Ring(query_weight, count, False)
    query_ring.step(1)
    first_chunk = call(
        pack_kernel,
        jax.ShapeDtypeStruct((rec_in_weight.shape[0], width + channels), BF16),
        [key_weight.T, value_weight.T, rec_in_weight],
    )
    first_ring = Ring(first_chunk, count, True)
    first_ring.step(1)
    shift = [(member, (member + 1) % count) for member in range(count)]
    halo = lax.ppermute(inputs[:, span - HALO // 2 :, :], "sp", shift)

    normed, gate_weights = call(
        norm_kernel,
        [
            jax.ShapeDtypeStruct((count, ext_rows, model_width // count), BF16),
            jax.ShapeDtypeStruct((channels, 2 * channels), BF16),
        ],
        [inputs, halo, norm_gain.reshape(1, model_width), decay_gate_weight, input_gate_weight],
    )
    out_weight = call(
        pack_out_kernel,
        [jax.ShapeDtypeStruct((att_width + channels, out_cols), BF16) for _ in range(tp_count)],
        [out_att_weight, out_rec_weight],
    )
    out_weight = [out_weight[0]] + [
        lax.ppermute(
            out_weight[member], "tp", [(source, source ^ member) for source in range(tp_count)]
        )
        for member in range(1, tp_count)
    ]

    for number in range(2, count // 2 + 1):
        first_ring.step(number)
        query_ring.step(number)
    gate_ring = Ring(rec_gate_weight, count, False)
    for number in range(1, count // 2 + 1):
        gate_ring.step(number)

    def part_of(ring):
        columns = ring.blocks[0].shape[1]
        return call(
            functools.partial(part_kernel, count),
            jax.ShapeDtypeStruct((ext_rows, columns), F32),
            [normed, *ring.blocks[:-1]],
        )

    message, local_state, cum_decay = call(
        functools.partial(recurrence_kernel, count, head_dim),
        [
            jax.ShapeDtypeStruct((rows + STATE_ROWS, width), BF16),
            jax.ShapeDtypeStruct((rows, channels), F32),
            jax.ShapeDtypeStruct((rows, channels), F32),
        ],
        [
            normed,
            part_of(first_ring),
            first_ring.blocks[-1],
            key_gain.reshape(1, head_dim),
            conv_weight,
            gate_weights,
            decay_param.reshape(1, channels),
            decay_extra,
        ],
        scratch=[pltpu.VMEM((ext_rows, channels), F32), pltpu.VMEM((8, width), F32)],
    )
    message_ring = Ring(message, count, True)
    for number in range(1, count // 2 + 1):
        message_ring.step(number)

    queries = call(
        functools.partial(query_kernel, count, head_dim, seq_count),
        jax.ShapeDtypeStruct((seq_count * heads, span, width), BF16),
        [normed, *query_ring.blocks, query_gain.reshape(1, head_dim)],
    )
    messages = message_ring.blocks
    rec_normed = call(
        functools.partial(entering_kernel, count, LRU_BLOCK),
        jax.ShapeDtypeStruct((rows, channels), BF16),
        [
            *messages,
            local_state,
            cum_decay,
            normed,
            part_of(gate_ring),
            gate_ring.blocks[-1],
            rec_out_gain.reshape(1, channels),
        ],
        scratch=[pltpu.VMEM((count, 8, width), F32)],
    )
    att_normed = call(
        functools.partial(attention_kernel, count, head_dim),
        jax.ShapeDtypeStruct((rows, att_width), BF16),
        [queries, *messages, forget_cache, attn_out_gain.reshape(1, att_width)],
        scratch=[pltpu.VMEM((count, heads * span, span), F32)],
    )

    def project(rec_members, att_members, base, kind):
        operands, uses = [], []
        weights = sorted({*rec_members, *att_members})
        for parts, half, members in ((rec_parts, 1, rec_members), (att_parts, 0, att_members)):
            for member in members:
                uses.append((len(operands), -1 - member, half))
                operands.append(parts[member])
        at_weight = {member: len(operands) + at for at, member in enumerate(weights)}
        uses = [(left, at_weight[-1 - right], half) for left, right, half in uses]
        operands += [out_weight[member] for member in weights]
        if base is not None:
            operands.append(base)
        return call(
            functools.partial(output_kernel, tuple(uses), base is not None),
            jax.ShapeDtypeStruct((rows, out_cols), kind),
            operands,
        )

    rec_parts = tp_spread(rec_normed, tp_count)
    att_parts = tp_spread(att_normed, tp_count)
    near, far = range(tp_count // 2), range(tp_count // 2, tp_count)
    base = project(range(tp_count), near, None, F32)
    mixed = project((), far, base, BF16)
    return mixed.reshape(seq_count, span, out_cols)


def fits(count, tp_count):
    return 4 <= count <= 16 and count % 2 == 0 and tp_count in (2, 4)


def layer(*arrays):
    inputs, query_weight, key_weight = arrays[0], arrays[2], arrays[3]
    head_dim, rec_in_weight = arrays[5].shape[0], arrays[8]
    count, tp_count = lax.axis_size("sp"), lax.axis_size("tp")
    whole_blocks = (
        inputs.shape[0] * rec_in_weight.shape[1] == 8 * head_dim
        and inputs.shape[1] == 2 * head_dim
        and key_weight.shape[1] == head_dim
        and query_weight.shape[1] == rec_in_weight.shape[1]
        and inputs.shape[2] % (128 * count) == 0
    )
    return (ring_body if fits(count, tp_count) and whole_blocks else body)(*arrays)


def solution(mesh):
    return jax.shard_map(
        layer,
        mesh=mesh,
        in_specs=(
            P(None, "sp", None),
            P(),
            P("sp", "tp"),
            P("sp", "tp"),
            P("sp", "tp"),
            P(),
            P(),
            P(None, "tp", None),
            P("sp", "tp"),
            P("sp", "tp"),
            P(None, "tp"),
            P("tp", None, None),
            P("tp", None, None),
            P("tp"),
            P(None, "sp", "tp"),
            P("tp"),
            P("tp"),
            P("tp", None),
            P("tp", None),
        ),
        out_specs=P(None, "sp", "tp"),
        check_vma=False,
    )
```

```python
import functools

import jax
import jax.numpy as jnp
from jax import lax
from jax.experimental import pallas as pl
from jax.experimental.pallas import tpu as pltpu
from jax.sharding import PartitionSpec as P

D = 2048
LRU_BLOCK = 64
CONV_TAPS = 4


lru_const = 8.0
norm_eps = 1e-06


def from_behind(value, axis, steps):
    count = lax.axis_size(axis)
    leading, last = (max(0, -steps), min(count, count - steps))
    return lax.ppermute(value, axis, [(source, source + steps) for source in range(leading, last)])


def rms_scale(values, gain):
    multiplier = lax.rsqrt(jnp.mean(values * values, axis=-1, keepdims=True) + norm_eps)
    return values * multiplier * gain


def merge_state(earlier, later):
    return (earlier[0] * later[0], later[0] * earlier[1] + later[1])


def block_length(length, span):
    shards = max(length // span, 1)
    group_size = 1
    for trial_size in range(1, shards + 1):
        if shards % trial_size == 0 and trial_size * span <= 1024:
            group_size = trial_size
    sub_size = group_size * span
    if length % sub_size:
        sub_size = length
    return sub_size


def body(
    inputs,
    norm_gain,
    query_weight,
    key_weight,
    value_weight,
    query_gain,
    key_gain,
    forget_cache,
    rec_in_weight,
    rec_gate_weight,
    conv_weight,
    decay_gate_weight,
    input_gate_weight,
    decay_param,
    decay_extra,
    attn_out_gain,
    rec_out_gain,
    out_att_weight,
    out_rec_weight,
):
    seq_count, seq_span, model_width = inputs.shape
    row_count = seq_count * seq_span
    head_dim = query_gain.shape[0]
    att_local = query_weight.shape[1] // head_dim
    kv_local = key_weight.shape[1] // head_dim
    head_group = att_local // kv_local
    channels = rec_in_weight.shape[1]
    normed = rms_scale(
        inputs.reshape(row_count, model_width).astype(jnp.float32), norm_gain
    ).astype(jnp.bfloat16)
    normed_cols = normed.T
    row_contract = (((0,), (0,)), ((), ()))
    kv_cols = key_weight.shape[1]
    pieces = (
        lax.all_gather(query_weight, "sp", axis=0, tiled=True),
        lax.all_gather(key_weight, "sp", axis=0, tiled=True),
        lax.all_gather(value_weight, "sp", axis=0, tiled=True),
        lax.all_gather(rec_in_weight, "sp", axis=0, tiled=True),
        lax.all_gather(rec_gate_weight, "sp", axis=0, tiled=True),
    )
    query_proj, key_proj, value_sum, rec_in_sum, gate_proj = tuple(
        (
            lax.dot_general(
                normed_cols, weight_part, row_contract, preferred_element_type=jnp.float32
            )
            for weight_part in pieces
        )
    )
    queries = rms_scale(query_proj.reshape(row_count, att_local, head_dim), query_gain).astype(
        jnp.bfloat16
    )
    queries = queries.reshape(seq_count, seq_span, kv_local, head_group, head_dim).transpose(
        0, 2, 3, 1, 4
    )
    queries = queries.reshape(seq_count, kv_local, head_group * seq_span, head_dim)
    key_heads = rms_scale(key_proj.reshape(row_count, kv_local, head_dim), key_gain).astype(
        jnp.bfloat16
    )
    key_heads = key_heads.reshape(seq_count, seq_span, kv_cols)
    value_heads = value_sum.astype(jnp.bfloat16).reshape(seq_count, seq_span, kv_cols)
    key_value = jnp.concatenate([key_heads, value_heads], axis=2)
    my_first = lax.axis_index("sp") * seq_span
    own_gates = lax.dynamic_slice_in_dim(forget_cache, my_first, seq_span, 2)
    own_gates = own_gates.reshape(seq_count, kv_local, head_group, seq_span, 1)
    query_pos = my_first + jnp.tile(jnp.arange(seq_span, dtype=jnp.int32), head_group)
    scaling = head_dim ** (-0.5)
    start_state = (
        jnp.full((seq_count, kv_local, head_group * seq_span), -jnp.inf, jnp.float32),
        jnp.zeros((seq_count, kv_local, head_group * seq_span), jnp.float32),
        jnp.zeros((seq_count, kv_local, head_group * seq_span, head_dim), jnp.float32),
    )
    shard_part = lax.all_gather(key_value, "sp", axis=1, tiled=True)
    offset = jnp.int32(0)
    length = shard_part.shape[1]
    sub_size = block_length(length, seq_span)

    def one_step(block_index, carried_state):
        key_first = offset + block_index * sub_size

        def work(carried):
            top_score, totals, accum = carried
            block_rows = lax.dynamic_slice_in_dim(shard_part, block_index * sub_size, sub_size, 1)
            key_block = block_rows[:, :, :kv_cols].reshape(seq_count, sub_size, kv_local, head_dim)
            value_block = block_rows[:, :, kv_cols:].reshape(
                seq_count, sub_size, kv_local, head_dim
            )
            key_gates = lax.dynamic_slice_in_dim(forget_cache, key_first, sub_size, 2)
            key_gates = key_gates.reshape(seq_count, kv_local, head_group, 1, sub_size)
            scores = (
                jnp.einsum(
                    "bhqd,bkhd->bhqk", queries, key_block, preferred_element_type=jnp.float32
                )
                * scaling
            )
            scores = (
                scores.reshape(seq_count, kv_local, head_group, seq_span, sub_size)
                + own_gates
                - key_gates
            )
            scores = scores.reshape(seq_count, kv_local, head_group * seq_span, sub_size)
            visible = (
                query_pos[:, None] >= (key_first + jnp.arange(sub_size, dtype=jnp.int32))[None, :]
            )
            scores = jnp.where(visible, scores, -jnp.inf)
            new_top = jnp.maximum(top_score, jnp.max(scores, axis=-1))
            safe_top = jnp.where(jnp.isfinite(new_top), new_top, 0.0)
            weights = jnp.exp(scores - safe_top[..., None])
            fading = jnp.exp(top_score - safe_top)
            totals = totals * fading + jnp.sum(weights, axis=-1)
            accum = accum * fading[..., None] + jnp.einsum(
                "bhqk,bkhd->bhqd",
                weights.astype(jnp.bfloat16),
                value_block,
                preferred_element_type=jnp.float32,
            )
            return (new_top, totals, accum)

        return lax.cond(
            key_first < my_first + seq_span, work, lambda carried: carried, carried_state
        )

    _, totals, accum = lax.fori_loop(0, length // sub_size, one_step, start_state)
    attended = (accum / totals[..., None]).reshape(
        seq_count, kv_local, head_group, seq_span, head_dim
    )
    attended = attended.transpose(0, 3, 1, 2, 4).reshape(row_count, att_local, head_dim)
    att_normed = rms_scale(attended, attn_out_gain.reshape(att_local, head_dim)).astype(
        jnp.bfloat16
    )
    att_normed = att_normed.reshape(row_count, att_local * head_dim)
    rec_in = rec_in_sum.astype(jnp.bfloat16).reshape(seq_count, seq_span, channels)
    before = from_behind(rec_in[:, seq_span - (CONV_TAPS - 1) :, :], "sp", 1)
    extended = jnp.concatenate([before, rec_in], axis=1)
    conv = jnp.zeros((seq_count, seq_span, channels), jnp.float32)
    for tap in range(CONV_TAPS):
        conv = conv + extended[:, tap : tap + seq_span].astype(jnp.float32) * conv_weight[
            tap
        ].astype(jnp.float32)
    conv = conv.astype(jnp.bfloat16)
    blocks_local = decay_gate_weight.shape[0]
    grouped = conv.reshape(seq_count, seq_span, blocks_local, LRU_BLOCK)
    gate_decay = jnp.einsum(
        "bsnd,nde->bsne", grouped, decay_gate_weight, preferred_element_type=jnp.float32
    ).reshape(seq_count, seq_span, channels)
    gate_input = jnp.einsum(
        "bsnd,nde->bsne", grouped, input_gate_weight, preferred_element_type=jnp.float32
    ).reshape(seq_count, seq_span, channels)
    log_decay = (
        -lru_const * jax.nn.sigmoid(gate_decay) * jax.nn.softplus(-decay_param) + decay_extra
    )
    drive = (
        jnp.sqrt(-jnp.expm1(2.0 * log_decay))
        * jax.nn.sigmoid(gate_input)
        * conv.astype(jnp.float32)
    )
    cum_decay, local_state = lax.associative_scan(merge_state, (jnp.exp(log_decay), drive), axis=1)
    every_decay, every_state = (
        lax.all_gather(cum_decay[:, seq_span - 1][None], "sp", axis=0, tiled=True),
        lax.all_gather(local_state[:, seq_span - 1][None], "sp", axis=0, tiled=True),
    )
    _, prefix_state = lax.associative_scan(merge_state, (every_decay, every_state), axis=0)
    position = lax.axis_index("sp")
    earlier_state = lax.dynamic_index_in_dim(
        prefix_state, jnp.maximum(position - 1, 0), 0, keepdims=False
    )
    entering = jnp.where(position > 0, earlier_state, 0.0)
    state = local_state + cum_decay * entering[:, None, :]
    gated = state * jax.nn.gelu(gate_proj.reshape(seq_count, seq_span, channels))
    rec_normed = rms_scale(
        gated.reshape(row_count, blocks_local, LRU_BLOCK),
        rec_out_gain.reshape(blocks_local, LRU_BLOCK),
    ).astype(jnp.bfloat16)
    rec_normed = rec_normed.reshape(row_count, channels)
    out_cols = D // lax.axis_size("tp")
    pieces = row_count * lax.axis_size("tp") // row_count
    terms = jnp.dot(att_normed, out_att_weight, preferred_element_type=jnp.float32) + jnp.dot(
        rec_normed, out_rec_weight, preferred_element_type=jnp.float32
    )
    mixed_cols = lax.psum_scatter(
        terms.reshape(row_count, pieces, out_cols)
        .transpose(1, 0, 2)
        .reshape(pieces * row_count, out_cols)
        .astype(jnp.bfloat16),
        "tp",
        scatter_dimension=0,
        tiled=True,
    )
    return mixed_cols.reshape(seq_count, seq_span, out_cols)


BF16 = jnp.bfloat16
F32 = jnp.float32
HALO = 8
STATE_ROWS = 32
KERNEL_VMEM = 10 << 20
BEGIN_FLOPS = 20_000_000_000
KERNEL_FLOPS = 4_000_000_000


def ring_positions(count):
    return list(range(0, count, 2)) + list(range(count - 1, 0, -2))


def arrivals(place, count):
    at = jnp.where(place % 2 == 0, place // 2, count - 1 - place // 2)

    def member(position):
        position = (position + count) % count
        return jnp.where(position < count // 2, 2 * position, 2 * (count - 1 - position) + 1)

    found = [place]
    for step in range(1, count // 2):
        found += [member(at - step), member(at + step)]
    return found + [member(at + count // 2)]


class Ring:
    def __init__(self, own, count, last_forward):
        order = ring_positions(count)
        self.count = count
        self.forward = [(order[at], order[(at + 1) % count]) for at in range(count)]
        self.backward = [(target, source) for source, target in self.forward]
        self.last_forward = last_forward
        self.blocks = [own]
        self.ahead = own
        self.behind = own

    def step(self, number):
        last = number == self.count // 2
        if not last or self.last_forward:
            self.ahead = lax.ppermute(self.ahead, "sp", self.forward)
            self.blocks.append(self.ahead)
        if not last or not self.last_forward:
            self.behind = lax.ppermute(self.behind, "sp", self.backward)
            self.blocks.append(self.behind)


def vmem():
    return pl.BlockSpec(memory_space=pltpu.VMEM)


def call(kernel, outs, operands, scratch=(), flops=KERNEL_FLOPS):
    single = not isinstance(outs, (list, tuple))
    return pl.pallas_call(
        kernel,
        out_shape=outs if single else tuple(outs),
        in_specs=[vmem()] * len(operands),
        out_specs=vmem() if single else tuple(vmem() for _ in outs),
        scratch_shapes=list(scratch),
        cost_estimate=pl.CostEstimate(flops=flops, bytes_accessed=0, transcendentals=0),
        compiler_params=pltpu.CompilerParams(vmem_limit_bytes=KERNEL_VMEM),
    )(*operands)


def block_diagonal(weight_ref):
    blocks, size, _ = weight_ref.shape
    tall = weight_ref[...].reshape(blocks * size, size)
    tiled = jnp.concatenate([tall] * blocks, axis=1)
    row = lax.broadcasted_iota(jnp.int32, tiled.shape, 0) // size
    column = lax.broadcasted_iota(jnp.int32, tiled.shape, 1) // size
    return jnp.where(row == column, tiled, jnp.zeros_like(tiled))


def begin_kernel(out_ref):
    out_ref[...] = jnp.zeros_like(out_ref)


def pack_kernel(_, key_ref, value_ref, rec_ref, out_ref):
    size = key_ref.shape[0]
    pair = jnp.concatenate([key_ref[...], value_ref[...]], axis=0)
    out_ref[:, : 2 * size] = pair.astype(F32).T.astype(BF16)
    out_ref[:, 2 * size :] = rec_ref[...]


TAP_ROW, RATE_ROW, REC_GAIN_ROW, ATT_GAIN_ROW, KEY_GAIN_ROW, QUERY_GAIN_ROW = 0, 8, 9, 10, 11, 12


def norm_kernel(rows_ref, gain_ref, decay_ref, input_ref, *refs):
    taps_ref, *line_refs = refs[:6]
    normed_ref, tail_ref, gates_ref, small_ref = refs[6:]
    small_ref[...] = jnp.zeros_like(small_ref)
    small_ref[TAP_ROW : TAP_ROW + CONV_TAPS, :] = taps_ref[...].astype(F32)
    for at, line_ref in enumerate(line_refs, RATE_ROW):
        copies = small_ref.shape[1] // line_ref.shape[1]
        small_ref[at : at + 1, :] = jnp.concatenate([line_ref[...]] * copies, axis=1)
    slices, _, width = normed_ref.shape
    seq_count, span, _ = rows_ref.shape
    gain = gain_ref[...]
    tails = []
    for seq in range(seq_count):
        values = rms_scale(rows_ref[seq].astype(F32), gain)
        tails.append(values[span - HALO :])
        normed = values.astype(BF16)
        for part in range(slices):
            normed_ref[part, seq * span : (seq + 1) * span, :] = normed[
                :, part * width : (part + 1) * width
            ]
    tail = jnp.concatenate(tails, axis=0).astype(BF16)
    for part in range(slices):
        tail_ref[part] = tail[:, part * width : (part + 1) * width]
    channels = gates_ref.shape[0]
    gates_ref[:, :channels] = block_diagonal(decay_ref)
    gates_ref[:, channels:] = block_diagonal(input_ref)


def pack_out_kernel(att_ref, rec_ref, *out_refs):
    place = lax.axis_index("tp")
    rows = att_ref.shape[0]
    for member, out_ref in enumerate(out_refs):
        width = out_ref.shape[1]
        columns = pl.ds(pl.multiple_of((place ^ member) * width, width), width)
        out_ref[:rows, :] = att_ref[:, columns]
        out_ref[rows:, :] = rec_ref[:, columns]


def softplus(value):
    small = jnp.exp(-jnp.abs(value))
    series = jnp.full_like(small, 1.0 / 7)
    for term in range(6, 0, -1):
        series = 1.0 / term - small * series
    return jnp.maximum(value, 0.0) + jnp.where(
        small < 0.05, small * series, jnp.log(1.0 + small)
    )


def gathered_dot(normed_ref, weight_refs, count, first=0, total=None, halo_ref=None):
    found = arrivals(lax.axis_index("sp"), count)[first:]
    for index, weight_ref in zip(found, weight_refs):
        rows = normed_ref[index]
        if halo_ref is not None:
            rows = jnp.concatenate([rows, halo_ref[index]], axis=0)
        term = jnp.dot(rows, weight_ref[...], preferred_element_type=F32)
        total = term if total is None else total + term
    return total


def part_kernel(count, with_halo, normed_ref, *refs):
    halo_ref = refs[0] if with_halo else None
    refs[-1][...] = gathered_dot(normed_ref, refs[with_halo:-1], count, halo_ref=halo_ref)


def minus_expm1(value, exp_value):
    series = jnp.full_like(value, 1.0)
    for term in range(9, 1, -1):
        series = 1.0 + value * (1.0 / term) * series
    return jnp.where(value > -0.5, -value * series, 1.0 - exp_value)


def shifted_down(value, steps, fill):
    moved = pltpu.roll(value, steps, 0)
    row = lax.broadcasted_iota(jnp.int32, value.shape, 0)
    return jnp.where(row >= steps, moved, fill)


def recurrence_kernel(count, head_dim, *refs):
    (
        normed_ref,
        halo_ref,
        part_ref,
        last_ref,
        small_ref,
        gates_ref,
        extra_ref,
        message_ref,
        state_ref,
        decay_ref,
        rec_ref,
        ends_ref,
    ) = refs
    seq_count, span, channels = extra_ref.shape
    kv_width = 2 * head_dim
    sums = gathered_dot(normed_ref, [last_ref], count, count - 1, part_ref[...], halo_ref)
    rec_in = sums[:, kv_width:].astype(BF16).astype(F32)
    kept = jnp.where(lax.axis_index("sp") > 0, 1.0, 0.0)
    rate = softplus(-small_ref[RATE_ROW : RATE_ROW + 1, :])
    taps = small_ref[TAP_ROW : TAP_ROW + CONV_TAPS, :]
    key_gain = small_ref[KEY_GAIN_ROW : KEY_GAIN_ROW + 1, :kv_width]
    lane = lax.broadcasted_iota(jnp.int32, (span, kv_width), 1)
    ends_ref[...] = jnp.zeros_like(ends_ref)
    halves = channels // kv_width
    for seq in range(seq_count):
        first = seq * (HALO + span)
        rows = pl.ds(seq * span, span)
        before = seq_count * span + seq * HALO
        rec_ref[first : first + HALO, :] = rec_in[before : before + HALO] * kept
        rec_ref[first + HALO : first + HALO + span, :] = rec_in[seq * span : (seq + 1) * span]
        kv = sums[seq * span : (seq + 1) * span, :kv_width]
        key = jnp.where(lane < head_dim, kv, 0.0)
        mean = jnp.sum(key * key, axis=-1, keepdims=True) * (1.0 / head_dim)
        scaled = kv * lax.rsqrt(mean + norm_eps) * key_gain
        message_ref[rows, :] = jnp.where(lane < head_dim, scaled, kv).astype(BF16)
        conv = jnp.zeros((span, channels), F32)
        for tap in range(CONV_TAPS):
            at = first + HALO - (CONV_TAPS - 1) + tap
            conv = conv + rec_ref[at : at + span, :] * taps[tap : tap + 1, :]
        conv = conv.astype(BF16)
        gated = jnp.dot(conv, gates_ref[...], preferred_element_type=F32)
        gate_decay, gate_input = gated[:, :channels], gated[:, channels:]
        log_decay = -lru_const * jax.nn.sigmoid(gate_decay) * rate + extra_ref[seq]
        decay = jnp.exp(log_decay)
        state = (
            jnp.sqrt(minus_expm1(2.0 * log_decay, decay * decay))
            * jax.nn.sigmoid(gate_input)
            * conv.astype(F32)
        )
        steps = 1
        while steps < span:
            state = state + decay * shifted_down(state, steps, 0.0)
            decay = decay * shifted_down(decay, steps, 1.0)
            steps *= 2
        state_ref[rows, :] = state
        decay_ref[rows, :] = decay
        for half in range(halves):
            lanes = slice(half * kv_width, (half + 1) * kv_width)
            at = seq * halves + half
            ends_ref[at : at + 1, :] = decay[span - 1 : span, lanes]
            at += seq_count * halves
            ends_ref[at : at + 1, :] = state[span - 1 : span, lanes]
    ends = ends_ref[...]
    high = ends.astype(BF16)
    left = ends - high.astype(F32)
    middle = left.astype(BF16)
    low = (left - middle.astype(F32)).astype(BF16)
    base = seq_count * span
    message_ref[base : base + 16, :] = jnp.concatenate([high, middle], axis=0)
    message_ref[base + 16 : base + 32, :] = jnp.concatenate([low, jnp.zeros_like(low)], axis=0)


def query_kernel(count, head_dim, seq_count, normed_ref, *refs):
    small_ref, query_ref = refs[-2:]
    width = query_ref.shape[2]
    span = query_ref.shape[1]
    heads = query_ref.shape[0] // seq_count
    gain = small_ref[QUERY_GAIN_ROW : QUERY_GAIN_ROW + 1, :width]
    sums = gathered_dot(normed_ref, refs[:-2], count)
    lane = lax.broadcasted_iota(jnp.int32, (span, width), 1)
    scaling = head_dim ** (-0.5)
    for seq in range(seq_count):
        rows = sums[seq * span : (seq + 1) * span]
        for head in range(heads):
            pair = rows[:, head // 2 * width : (head // 2 + 1) * width]
            if head % 2:
                pair = pltpu.roll(pair, head_dim, 1)
            own = jnp.where(lane < head_dim, pair, 0.0)
            mean = jnp.sum(own * own, axis=-1, keepdims=True) * (1.0 / head_dim)
            scaled = (own * lax.rsqrt(mean + norm_eps) * gain).astype(BF16)
            query_ref[seq * heads + head] = scaled * jnp.asarray(scaling, BF16)


def entering_kernel(count, group, *refs):
    place = lax.axis_index("sp")
    message_refs = refs[:count]
    (
        state_ref,
        decay_ref,
        normed_ref,
        part_ref,
        last_ref,
        small_ref,
        out_ref,
        ends_ref,
    ) = refs[count:]
    gate = gathered_dot(normed_ref, [last_ref], count, count - 1, part_ref[...])
    rows, channels = state_ref.shape
    width = ends_ref.shape[2]
    halves = channels // width
    seq_count = ends_ref.shape[1] // (2 * halves)
    span = rows // seq_count
    for index, message_ref in zip(arrivals(place, count), message_refs):
        parts = message_ref[rows:, :].astype(F32)
        ends_ref[index] = parts[0:8] + parts[8:16] + parts[16:24]
    half_rows = seq_count * halves
    entering = jnp.zeros((half_rows, width), F32)
    for earlier in range(count - 1):
        ends = ends_ref[earlier]
        merged = ends[:half_rows] * entering + ends[half_rows:]
        entering = jnp.where(earlier < place, merged, entering)
    lane = lax.broadcasted_iota(jnp.int32, (span, width), 1)
    for seq in range(seq_count):
        for half in range(halves):
            lanes = slice(half * width, (half + 1) * width)
            at = seq * halves + half
            part = pl.ds(seq * span, span)
            first = seq * span
            state = state_ref[part, lanes] + decay_ref[part, lanes] * entering[at : at + 1, :]
            gated = state * jax.nn.gelu(gate[first : first + span, lanes])
            square = gated * gated
            total = jnp.sum(square, axis=-1, keepdims=True)
            low = jnp.sum(jnp.where(lane < group, square, 0.0), axis=-1, keepdims=True)
            mean = jnp.where(lane < group, low, total - low) * (1.0 / group)
            out_ref[part, lanes] = (
                gated * lax.rsqrt(mean + norm_eps) * small_ref[REC_GAIN_ROW : REC_GAIN_ROW + 1, lanes]
            ).astype(BF16)


def lane_sums(value, first=0):
    lanes = value.shape[1]
    row = lax.broadcasted_iota(jnp.int32, (lanes, lanes), 0)
    chosen = jnp.where(row >= first, 1.0, 0.0).astype(BF16)
    high = value.astype(BF16)
    low = (value - high.astype(F32)).astype(BF16)
    return jnp.dot(high, chosen, preferred_element_type=F32) + jnp.dot(
        low, chosen, preferred_element_type=F32
    )


def attention_kernel(count, head_dim, first, last, *refs):
    query_ref = refs[0]
    message_refs = refs[1 : 1 + last - first]
    refs = refs[1 + last - first :]
    gate_ref = refs[0]
    before_refs = refs[1:4] if first else None
    score_ref = refs[-1]
    if last == count:
        small_ref, out_ref = refs[-3:-1]
    else:
        after_refs = refs[-4:-1]
    span, width = query_ref.shape[1:]
    seq_count = gate_ref.shape[0]
    heads = query_ref.shape[0] // seq_count
    place = lax.axis_index("sp")
    found = arrivals(place, count)[first:last]
    ahead = lax.broadcasted_iota(jnp.int32, (span, span), 1) - lax.broadcasted_iota(
        jnp.int32, (span, span), 0
    )
    lane = lax.broadcasted_iota(jnp.int32, (span, width), 1)
    for seq in range(seq_count):
        keys = pl.ds(seq * span, span)
        lines = [
            slice((seq * heads + head) * span, (seq * heads + head + 1) * span)
            for head in range(heads)
        ]
        queries = query_ref[seq * heads : (seq + 1) * heads].reshape(heads * span, width)
        top = [None] * heads
        own = gate_ref[seq, :, pl.ds(pl.multiple_of(place * span, span), span)]
        own = jnp.concatenate([own, jnp.zeros((span - heads, span), F32)], axis=0).T
        for at, block in enumerate(found):
            scores = lax.dot_general(
                queries,
                message_refs[at][keys, :],
                (((1,), (1,)), ((), ())),
                preferred_element_type=F32,
            )
            hidden = ahead > (place - block) * span
            gates = gate_ref[seq, :, pl.ds(pl.multiple_of(block * span, span), span)]
            for head in range(heads):
                score = scores[head * span : (head + 1) * span]
                score = score + own[:, head : head + 1] - gates[head : head + 1, :]
                score = jnp.where(hidden, -jnp.inf, score)
                score_ref[at, head * span : (head + 1) * span, :] = score
                top[head] = score if at == 0 else jnp.maximum(top[head], score)
        top = [jnp.max(part, axis=-1, keepdims=True) for part in top]
        if first:
            top_before = [before_refs[0][line, :] for line in lines]
            top = [jnp.maximum(part, old) for part, old in zip(top, top_before)]
        totals = [None] * heads
        weighted = None
        for at in range(len(found)):
            weights = []
            for head in range(heads):
                part = jnp.exp(score_ref[at, head * span : (head + 1) * span, :] - top[head])
                totals[head] = part if at == 0 else totals[head] + part
                weights.append(part.astype(BF16))
            term = jnp.dot(
                jnp.concatenate(weights, axis=0),
                message_refs[at][keys, :],
                preferred_element_type=F32,
            )
            weighted = term if at == 0 else weighted + term
        outs = []
        for head in range(heads):
            total = lane_sums(totals[head])
            value = weighted[head * span : (head + 1) * span]
            line = lines[head]
            if first:
                fading = jnp.exp(top_before[head] - top[head])
                total = total + before_refs[1][line, :] * fading
                value = value + before_refs[2][line, :] * fading
            if last < count:
                after_refs[0][line, :] = jnp.broadcast_to(top[head], value.shape)
                after_refs[1][line, :] = total
                after_refs[2][line, :] = value
                continue
            attended = value * (1.0 / total)
            mean = lane_sums(attended * attended, head_dim) * (1.0 / head_dim)
            outs.append(attended * lax.rsqrt(mean + norm_eps))
        for pair in range(len(outs) // 2):
            lanes = slice(pair * width, (pair + 1) * width)
            joined = jnp.where(
                lane < head_dim, pltpu.roll(outs[2 * pair], head_dim, 1), outs[2 * pair + 1]
            )
            gain = small_ref[ATT_GAIN_ROW : ATT_GAIN_ROW + 1, lanes]
            out_ref[keys, lanes] = (joined * gain).astype(BF16)


def output_kernel(uses, has_base, *refs):
    out_ref = refs[-1]
    total = refs[-2][...] if has_base else None
    for left, right, half in uses:
        rows = refs[left].shape[1]
        term = jnp.dot(
            refs[left][...],
            refs[right][half * rows : (half + 1) * rows, :],
            preferred_element_type=F32,
        )
        total = term if total is None else total + term
    out_ref[...] = total.astype(out_ref.dtype)


def tp_spread(value, count):
    bits = [1 << at for at in range(count.bit_length() - 1)]
    found = {0: value}
    for bit in reversed(bits):
        pairs = [(source, source ^ bit) for source in range(count)]
        for member in sorted(found):
            found[member ^ bit] = lax.ppermute(found[member], "tp", pairs)
    return [found[member] for member in range(count)]


def ring_body(
    inputs,
    norm_gain,
    query_weight,
    key_weight,
    value_weight,
    query_gain,
    key_gain,
    forget_cache,
    rec_in_weight,
    rec_gate_weight,
    conv_weight,
    decay_gate_weight,
    input_gate_weight,
    decay_param,
    decay_extra,
    attn_out_gain,
    rec_out_gain,
    out_att_weight,
    out_rec_weight,
):
    count = lax.axis_size("sp")
    tp_count = lax.axis_size("tp")
    seq_count, span, model_width = inputs.shape
    rows = seq_count * span
    head_dim = query_gain.shape[0]
    width = 2 * head_dim
    att_width = query_weight.shape[1]
    heads = att_width // head_dim
    channels = rec_in_weight.shape[1]
    ext_rows = seq_count * (HALO + span)
    out_cols = model_width // tp_count
    query_ring = Ring(query_weight, count, False)
    query_ring.step(1)
    begun = call(begin_kernel, jax.ShapeDtypeStruct((8, 128), F32), [], flops=BEGIN_FLOPS)
    first_chunk = call(
        pack_kernel,
        jax.ShapeDtypeStruct((rec_in_weight.shape[0], width + channels), BF16),
        [begun, key_weight.T, value_weight.T, rec_in_weight],
    )
    first_ring = Ring(first_chunk, count, True)
    first_ring.step(1)
    slice_width = model_width // count
    normed, tail, gate_weights, small = call(
        norm_kernel,
        [
            jax.ShapeDtypeStruct((count, rows, slice_width), BF16),
            jax.ShapeDtypeStruct((count, seq_count * HALO, slice_width), BF16),
            jax.ShapeDtypeStruct((channels, 2 * channels), BF16),
            jax.ShapeDtypeStruct((16, channels), F32),
        ],
        [
            inputs,
            norm_gain.reshape(1, model_width),
            decay_gate_weight,
            input_gate_weight,
            conv_weight,
            decay_param.reshape(1, channels),
            rec_out_gain.reshape(1, channels),
            attn_out_gain.reshape(1, att_width),
            key_gain.reshape(1, head_dim),
            query_gain.reshape(1, head_dim),
        ],
    )
    out_weight = list(
        call(
            pack_out_kernel,
            [jax.ShapeDtypeStruct((att_width + channels, out_cols), BF16)] * tp_count,
            [out_att_weight, out_rec_weight],
        )
    )
    shift = [(member, (member + 1) % count) for member in range(count)]
    halo = lax.ppermute(tail, "sp", shift)
    for member in range(1, tp_count):
        pairs = [(source, source ^ member) for source in range(tp_count)]
        out_weight[member] = lax.ppermute(out_weight[member], "tp", pairs)

    for number in range(2, count // 2 + 1):
        first_ring.step(number)
        query_ring.step(number)
    gate_ring = Ring(rec_gate_weight, count, False)
    for number in range(1, count // 2 + 1):
        gate_ring.step(number)

    def part_of(ring, halos=()):
        columns = ring.blocks[0].shape[1]
        return call(
            functools.partial(part_kernel, count, len(halos)),
            jax.ShapeDtypeStruct((rows + len(halos) * seq_count * HALO, columns), F32),
            [normed, *halos, *ring.blocks[:-1]],
        )

    message, local_state, cum_decay = call(
        functools.partial(recurrence_kernel, count, head_dim),
        [
            jax.ShapeDtypeStruct((rows + STATE_ROWS, width), BF16),
            jax.ShapeDtypeStruct((rows, channels), F32),
            jax.ShapeDtypeStruct((rows, channels), F32),
        ],
        [
            normed,
            halo,
            part_of(first_ring, (halo,)),
            first_ring.blocks[-1],
            small,
            gate_weights,
            decay_extra,
        ],
        scratch=[pltpu.VMEM((ext_rows, channels), F32), pltpu.VMEM((8, width), F32)],
    )
    message_ring = Ring(message, count, True)
    for number in range(1, count // 2 + 1):
        message_ring.step(number)

    queries = call(
        functools.partial(query_kernel, count, head_dim, seq_count),
        jax.ShapeDtypeStruct((seq_count * heads, span, width), BF16),
        [normed, *query_ring.blocks, small],
    )
    messages = message_ring.blocks
    rec_normed = call(
        functools.partial(entering_kernel, count, LRU_BLOCK),
        jax.ShapeDtypeStruct((rows, channels), BF16),
        [
            *messages,
            local_state,
            cum_decay,
            normed,
            part_of(gate_ring),
            gate_ring.blocks[-1],
            small,
        ],
        scratch=[pltpu.VMEM((count, 8, width), F32)],
    )
    early = count - 1
    attended = call(
        functools.partial(attention_kernel, count, head_dim, 0, early),
        [jax.ShapeDtypeStruct((seq_count * heads * span, width), F32)] * 3,
        [queries, *messages[:early], forget_cache],
        scratch=[pltpu.VMEM((early, heads * span, span), F32)],
    )
    att_normed = call(
        functools.partial(attention_kernel, count, head_dim, early, count),
        jax.ShapeDtypeStruct((rows, att_width), BF16),
        [queries, *messages[early:], forget_cache, *attended, small],
        scratch=[pltpu.VMEM((count - early, heads * span, span), F32)],
    )

    def project(rec_members, att_members, base, kind):
        operands, uses = [], []
        weights = sorted({*rec_members, *att_members})
        for parts, half, members in ((rec_parts, 1, rec_members), (att_parts, 0, att_members)):
            for member in members:
                uses.append((len(operands), -1 - member, half))
                operands.append(parts[member])
        at_weight = {member: len(operands) + at for at, member in enumerate(weights)}
        uses = [(left, at_weight[-1 - right], half) for left, right, half in uses]
        operands += [out_weight[member] for member in weights]
        if base is not None:
            operands.append(base)
        return call(
            functools.partial(output_kernel, tuple(uses), base is not None),
            jax.ShapeDtypeStruct((rows, out_cols), kind),
            operands,
        )

    rec_parts = tp_spread(rec_normed, tp_count)
    att_parts = tp_spread(att_normed, tp_count)
    near, far = range(tp_count // 2), range(tp_count // 2, tp_count)
    base = project(range(tp_count), near, None, F32)
    mixed = project((), far, base, BF16)
    return mixed.reshape(seq_count, span, out_cols)


def fits(count, tp_count):
    return 4 <= count <= 16 and count % 2 == 0 and tp_count in (2, 4)


def layer(*arrays):
    inputs, query_weight, key_weight = arrays[0], arrays[2], arrays[3]
    head_dim, rec_in_weight = arrays[5].shape[0], arrays[8]
    count, tp_count = lax.axis_size("sp"), lax.axis_size("tp")
    whole_blocks = (
        inputs.shape[0] * rec_in_weight.shape[1] == 8 * head_dim
        and inputs.shape[1] == 2 * head_dim
        and key_weight.shape[1] == head_dim
        and query_weight.shape[1] == rec_in_weight.shape[1]
        and inputs.shape[2] % (128 * count) == 0
    )
    return (ring_body if fits(count, tp_count) and whole_blocks else body)(*arrays)


def solution(mesh):
    return jax.shard_map(
        layer,
        mesh=mesh,
        in_specs=(
            P(None, "sp", None),
            P(),
            P("sp", "tp"),
            P("sp", "tp"),
            P("sp", "tp"),
            P(),
            P(),
            P(None, "tp", None),
            P("sp", "tp"),
            P("sp", "tp"),
            P(None, "tp"),
            P("tp", None, None),
            P("tp", None, None),
            P("tp"),
            P(None, "sp", "tp"),
            P("tp"),
            P("tp"),
            P("tp", None),
            P("tp", None),
        ),
        out_specs=P(None, "sp", "tp"),
        check_vma=False,
    )
```

```python
import functools

import jax
import jax.numpy as jnp
from jax import lax
from jax.experimental import pallas as pl
from jax.experimental.pallas import tpu as pltpu
from jax.sharding import PartitionSpec as P

D = 2048
LRU_BLOCK = 64
CONV_TAPS = 4


lru_const = 8.0
norm_eps = 1e-06


def from_behind(value, axis, steps):
    count = lax.axis_size(axis)
    leading, last = (max(0, -steps), min(count, count - steps))
    return lax.ppermute(value, axis, [(source, source + steps) for source in range(leading, last)])


def rms_scale(values, gain):
    multiplier = lax.rsqrt(jnp.mean(values * values, axis=-1, keepdims=True) + norm_eps)
    return values * multiplier * gain


def merge_state(earlier, later):
    return (earlier[0] * later[0], later[0] * earlier[1] + later[1])


def block_length(length, span):
    shards = max(length // span, 1)
    group_size = 1
    for trial_size in range(1, shards + 1):
        if shards % trial_size == 0 and trial_size * span <= 1024:
            group_size = trial_size
    sub_size = group_size * span
    if length % sub_size:
        sub_size = length
    return sub_size


def body(
    inputs,
    norm_gain,
    query_weight,
    key_weight,
    value_weight,
    query_gain,
    key_gain,
    forget_cache,
    rec_in_weight,
    rec_gate_weight,
    conv_weight,
    decay_gate_weight,
    input_gate_weight,
    decay_param,
    decay_extra,
    attn_out_gain,
    rec_out_gain,
    out_att_weight,
    out_rec_weight,
):
    seq_count, seq_span, model_width = inputs.shape
    row_count = seq_count * seq_span
    head_dim = query_gain.shape[0]
    att_local = query_weight.shape[1] // head_dim
    kv_local = key_weight.shape[1] // head_dim
    head_group = att_local // kv_local
    channels = rec_in_weight.shape[1]
    normed = rms_scale(
        inputs.reshape(row_count, model_width).astype(jnp.float32), norm_gain
    ).astype(jnp.bfloat16)
    normed_cols = normed.T
    row_contract = (((0,), (0,)), ((), ()))
    kv_cols = key_weight.shape[1]
    pieces = (
        lax.all_gather(query_weight, "sp", axis=0, tiled=True),
        lax.all_gather(key_weight, "sp", axis=0, tiled=True),
        lax.all_gather(value_weight, "sp", axis=0, tiled=True),
        lax.all_gather(rec_in_weight, "sp", axis=0, tiled=True),
        lax.all_gather(rec_gate_weight, "sp", axis=0, tiled=True),
    )
    query_proj, key_proj, value_sum, rec_in_sum, gate_proj = tuple(
        (
            lax.dot_general(
                normed_cols, weight_part, row_contract, preferred_element_type=jnp.float32
            )
            for weight_part in pieces
        )
    )
    queries = rms_scale(query_proj.reshape(row_count, att_local, head_dim), query_gain).astype(
        jnp.bfloat16
    )
    queries = queries.reshape(seq_count, seq_span, kv_local, head_group, head_dim).transpose(
        0, 2, 3, 1, 4
    )
    queries = queries.reshape(seq_count, kv_local, head_group * seq_span, head_dim)
    key_heads = rms_scale(key_proj.reshape(row_count, kv_local, head_dim), key_gain).astype(
        jnp.bfloat16
    )
    key_heads = key_heads.reshape(seq_count, seq_span, kv_cols)
    value_heads = value_sum.astype(jnp.bfloat16).reshape(seq_count, seq_span, kv_cols)
    key_value = jnp.concatenate([key_heads, value_heads], axis=2)
    my_first = lax.axis_index("sp") * seq_span
    own_gates = lax.dynamic_slice_in_dim(forget_cache, my_first, seq_span, 2)
    own_gates = own_gates.reshape(seq_count, kv_local, head_group, seq_span, 1)
    query_pos = my_first + jnp.tile(jnp.arange(seq_span, dtype=jnp.int32), head_group)
    scaling = head_dim ** (-0.5)
    start_state = (
        jnp.full((seq_count, kv_local, head_group * seq_span), -jnp.inf, jnp.float32),
        jnp.zeros((seq_count, kv_local, head_group * seq_span), jnp.float32),
        jnp.zeros((seq_count, kv_local, head_group * seq_span, head_dim), jnp.float32),
    )
    shard_part = lax.all_gather(key_value, "sp", axis=1, tiled=True)
    offset = jnp.int32(0)
    length = shard_part.shape[1]
    sub_size = block_length(length, seq_span)

    def one_step(block_index, carried_state):
        key_first = offset + block_index * sub_size

        def work(carried):
            top_score, totals, accum = carried
            block_rows = lax.dynamic_slice_in_dim(shard_part, block_index * sub_size, sub_size, 1)
            key_block = block_rows[:, :, :kv_cols].reshape(seq_count, sub_size, kv_local, head_dim)
            value_block = block_rows[:, :, kv_cols:].reshape(
                seq_count, sub_size, kv_local, head_dim
            )
            key_gates = lax.dynamic_slice_in_dim(forget_cache, key_first, sub_size, 2)
            key_gates = key_gates.reshape(seq_count, kv_local, head_group, 1, sub_size)
            scores = (
                jnp.einsum(
                    "bhqd,bkhd->bhqk", queries, key_block, preferred_element_type=jnp.float32
                )
                * scaling
            )
            scores = (
                scores.reshape(seq_count, kv_local, head_group, seq_span, sub_size)
                + own_gates
                - key_gates
            )
            scores = scores.reshape(seq_count, kv_local, head_group * seq_span, sub_size)
            visible = (
                query_pos[:, None] >= (key_first + jnp.arange(sub_size, dtype=jnp.int32))[None, :]
            )
            scores = jnp.where(visible, scores, -jnp.inf)
            new_top = jnp.maximum(top_score, jnp.max(scores, axis=-1))
            safe_top = jnp.where(jnp.isfinite(new_top), new_top, 0.0)
            weights = jnp.exp(scores - safe_top[..., None])
            fading = jnp.exp(top_score - safe_top)
            totals = totals * fading + jnp.sum(weights, axis=-1)
            accum = accum * fading[..., None] + jnp.einsum(
                "bhqk,bkhd->bhqd",
                weights.astype(jnp.bfloat16),
                value_block,
                preferred_element_type=jnp.float32,
            )
            return (new_top, totals, accum)

        return lax.cond(
            key_first < my_first + seq_span, work, lambda carried: carried, carried_state
        )

    _, totals, accum = lax.fori_loop(0, length // sub_size, one_step, start_state)
    attended = (accum / totals[..., None]).reshape(
        seq_count, kv_local, head_group, seq_span, head_dim
    )
    attended = attended.transpose(0, 3, 1, 2, 4).reshape(row_count, att_local, head_dim)
    att_normed = rms_scale(attended, attn_out_gain.reshape(att_local, head_dim)).astype(
        jnp.bfloat16
    )
    att_normed = att_normed.reshape(row_count, att_local * head_dim)
    rec_in = rec_in_sum.astype(jnp.bfloat16).reshape(seq_count, seq_span, channels)
    before = from_behind(rec_in[:, seq_span - (CONV_TAPS - 1) :, :], "sp", 1)
    extended = jnp.concatenate([before, rec_in], axis=1)
    conv = jnp.zeros((seq_count, seq_span, channels), jnp.float32)
    for tap in range(CONV_TAPS):
        conv = conv + extended[:, tap : tap + seq_span].astype(jnp.float32) * conv_weight[
            tap
        ].astype(jnp.float32)
    conv = conv.astype(jnp.bfloat16)
    blocks_local = decay_gate_weight.shape[0]
    grouped = conv.reshape(seq_count, seq_span, blocks_local, LRU_BLOCK)
    gate_decay = jnp.einsum(
        "bsnd,nde->bsne", grouped, decay_gate_weight, preferred_element_type=jnp.float32
    ).reshape(seq_count, seq_span, channels)
    gate_input = jnp.einsum(
        "bsnd,nde->bsne", grouped, input_gate_weight, preferred_element_type=jnp.float32
    ).reshape(seq_count, seq_span, channels)
    log_decay = (
        -lru_const * jax.nn.sigmoid(gate_decay) * jax.nn.softplus(-decay_param) + decay_extra
    )
    drive = (
        jnp.sqrt(-jnp.expm1(2.0 * log_decay))
        * jax.nn.sigmoid(gate_input)
        * conv.astype(jnp.float32)
    )
    cum_decay, local_state = lax.associative_scan(merge_state, (jnp.exp(log_decay), drive), axis=1)
    every_decay, every_state = (
        lax.all_gather(cum_decay[:, seq_span - 1][None], "sp", axis=0, tiled=True),
        lax.all_gather(local_state[:, seq_span - 1][None], "sp", axis=0, tiled=True),
    )
    _, prefix_state = lax.associative_scan(merge_state, (every_decay, every_state), axis=0)
    position = lax.axis_index("sp")
    earlier_state = lax.dynamic_index_in_dim(
        prefix_state, jnp.maximum(position - 1, 0), 0, keepdims=False
    )
    entering = jnp.where(position > 0, earlier_state, 0.0)
    state = local_state + cum_decay * entering[:, None, :]
    gated = state * jax.nn.gelu(gate_proj.reshape(seq_count, seq_span, channels))
    rec_normed = rms_scale(
        gated.reshape(row_count, blocks_local, LRU_BLOCK),
        rec_out_gain.reshape(blocks_local, LRU_BLOCK),
    ).astype(jnp.bfloat16)
    rec_normed = rec_normed.reshape(row_count, channels)
    out_cols = D // lax.axis_size("tp")
    pieces = row_count * lax.axis_size("tp") // row_count
    terms = jnp.dot(att_normed, out_att_weight, preferred_element_type=jnp.float32) + jnp.dot(
        rec_normed, out_rec_weight, preferred_element_type=jnp.float32
    )
    mixed_cols = lax.psum_scatter(
        terms.reshape(row_count, pieces, out_cols)
        .transpose(1, 0, 2)
        .reshape(pieces * row_count, out_cols)
        .astype(jnp.bfloat16),
        "tp",
        scatter_dimension=0,
        tiled=True,
    )
    return mixed_cols.reshape(seq_count, seq_span, out_cols)


BF16 = jnp.bfloat16
F32 = jnp.float32
HALO = 8
STATE_ROWS = 32
KERNEL_VMEM = 10 << 20
BEGIN_FLOPS = 20_000_000_000
KERNEL_FLOPS = 4_000_000_000


def ring_positions(count):
    return list(range(0, count, 2)) + list(range(count - 1, 0, -2))


def arrivals(place, count):
    at = jnp.where(place % 2 == 0, place // 2, count - 1 - place // 2)

    def member(position):
        position = (position + count) % count
        return jnp.where(position < count // 2, 2 * position, 2 * (count - 1 - position) + 1)

    found = [place]
    for step in range(1, count // 2):
        found += [member(at - step), member(at + step)]
    return found + [member(at + count // 2)]


class Ring:
    def __init__(self, own, count, last_forward):
        order = ring_positions(count)
        self.count = count
        self.forward = [(order[at], order[(at + 1) % count]) for at in range(count)]
        self.backward = [(target, source) for source, target in self.forward]
        self.last_forward = last_forward
        self.blocks = [own]
        self.ahead = own
        self.behind = own

    def step(self, number):
        last = number == self.count // 2
        if not last or self.last_forward:
            self.ahead = lax.ppermute(self.ahead, "sp", self.forward)
            self.blocks.append(self.ahead)
        if not last or not self.last_forward:
            self.behind = lax.ppermute(self.behind, "sp", self.backward)
            self.blocks.append(self.behind)


def vmem():
    return pl.BlockSpec(memory_space=pltpu.VMEM)


def call(kernel, outs, operands, scratch=(), flops=KERNEL_FLOPS):
    single = not isinstance(outs, (list, tuple))
    return pl.pallas_call(
        kernel,
        out_shape=outs if single else tuple(outs),
        in_specs=[vmem()] * len(operands),
        out_specs=vmem() if single else tuple(vmem() for _ in outs),
        scratch_shapes=list(scratch),
        cost_estimate=pl.CostEstimate(flops=flops, bytes_accessed=0, transcendentals=0),
        compiler_params=pltpu.CompilerParams(vmem_limit_bytes=KERNEL_VMEM),
    )(*operands)


def block_diagonal(weight_ref):
    blocks, size, _ = weight_ref.shape
    tall = weight_ref[...].reshape(blocks * size, size)
    tiled = jnp.concatenate([tall] * blocks, axis=1)
    row = lax.broadcasted_iota(jnp.int32, tiled.shape, 0) // size
    column = lax.broadcasted_iota(jnp.int32, tiled.shape, 1) // size
    return jnp.where(row == column, tiled, jnp.zeros_like(tiled))


def begin_kernel(out_ref):
    out_ref[...] = jnp.zeros_like(out_ref)


def pack_kernel(_, key_ref, value_ref, rec_ref, out_ref):
    size = key_ref.shape[0]
    pair = jnp.concatenate([key_ref[...], value_ref[...]], axis=0)
    out_ref[:, : 2 * size] = pair.astype(F32).T.astype(BF16)
    out_ref[:, 2 * size :] = rec_ref[...]


TAP_ROW, RATE_ROW, REC_GAIN_ROW, ATT_GAIN_ROW, KEY_GAIN_ROW, QUERY_GAIN_ROW = 0, 8, 9, 10, 11, 12


def norm_kernel(rows_ref, gain_ref, decay_ref, input_ref, *refs):
    taps_ref, *line_refs = refs[:6]
    normed_ref, tail_ref, gates_ref, small_ref = refs[6:]
    small_ref[...] = jnp.zeros_like(small_ref)
    small_ref[TAP_ROW : TAP_ROW + CONV_TAPS, :] = taps_ref[...].astype(F32)
    for at, line_ref in enumerate(line_refs, RATE_ROW):
        copies = small_ref.shape[1] // line_ref.shape[1]
        small_ref[at : at + 1, :] = jnp.concatenate([line_ref[...]] * copies, axis=1)
    slices, _, width = normed_ref.shape
    seq_count, span, _ = rows_ref.shape
    gain = gain_ref[...]
    tails = []
    for seq in range(seq_count):
        values = rms_scale(rows_ref[seq].astype(F32), gain)
        tails.append(values[span - HALO // seq_count :])
        normed = values.astype(BF16)
        for part in range(slices):
            normed_ref[part, seq * span : (seq + 1) * span, :] = normed[
                :, part * width : (part + 1) * width
            ]
    tail = jnp.concatenate(tails, axis=0).astype(BF16)
    for part in range(slices):
        tail_ref[part] = tail[:, part * width : (part + 1) * width]
    channels = gates_ref.shape[0]
    gates_ref[:, :channels] = block_diagonal(decay_ref)
    gates_ref[:, channels:] = block_diagonal(input_ref)


def pack_out_kernel(att_ref, rec_ref, *out_refs):
    place = lax.axis_index("tp")
    rows = att_ref.shape[0]
    for member, out_ref in enumerate(out_refs):
        width = out_ref.shape[1]
        columns = pl.ds(pl.multiple_of((place ^ member) * width, width), width)
        out_ref[:rows, :] = att_ref[:, columns]
        out_ref[rows:, :] = rec_ref[:, columns]


def softplus(value):
    small = jnp.exp(-jnp.abs(value))
    series = jnp.full_like(small, 1.0 / 7)
    for term in range(6, 0, -1):
        series = 1.0 / term - small * series
    return jnp.maximum(value, 0.0) + jnp.where(
        small < 0.05, small * series, jnp.log(1.0 + small)
    )


def gathered_dot(normed_ref, weight_refs, count, first=0, total=None, halo_ref=None):
    found = arrivals(lax.axis_index("sp"), count)[first:]
    for index, weight_ref in zip(found, weight_refs):
        rows = normed_ref[index]
        if halo_ref is not None:
            rows = jnp.concatenate([rows, halo_ref[index]], axis=0)
        term = jnp.dot(rows, weight_ref[...], preferred_element_type=F32)
        total = term if total is None else total + term
    return total


def part_kernel(count, with_halo, normed_ref, *refs):
    halo_ref = refs[0] if with_halo else None
    refs[-1][...] = gathered_dot(normed_ref, refs[with_halo:-1], count, halo_ref=halo_ref)


def minus_expm1(value, exp_value):
    series = jnp.full_like(value, 1.0)
    for term in range(9, 1, -1):
        series = 1.0 + value * (1.0 / term) * series
    return jnp.where(value > -0.5, -value * series, 1.0 - exp_value)


def shifted_down(value, steps, fill):
    moved = pltpu.roll(value, steps, 0)
    row = lax.broadcasted_iota(jnp.int32, value.shape, 0)
    return jnp.where(row >= steps, moved, fill)


def recurrence_kernel(count, head_dim, *refs):
    (
        normed_ref,
        halo_ref,
        part_ref,
        last_ref,
        small_ref,
        gates_ref,
        extra_ref,
        message_ref,
        state_ref,
        decay_ref,
        rec_ref,
        ends_ref,
    ) = refs
    seq_count, span, channels = extra_ref.shape
    kv_width = 2 * head_dim
    sums = gathered_dot(normed_ref, [last_ref], count, count - 1, part_ref[...], halo_ref)
    rec_in = sums[:, kv_width:].astype(BF16).astype(F32)
    kept = jnp.where(lax.axis_index("sp") > 0, 1.0, 0.0)
    rate = softplus(-small_ref[RATE_ROW : RATE_ROW + 1, :])
    taps = small_ref[TAP_ROW : TAP_ROW + CONV_TAPS, :]
    key_gain = small_ref[KEY_GAIN_ROW : KEY_GAIN_ROW + 1, :kv_width]
    lane = lax.broadcasted_iota(jnp.int32, (span, kv_width), 1)
    ends_ref[...] = jnp.zeros_like(ends_ref)
    halves = channels // kv_width
    for seq in range(seq_count):
        first = seq * (HALO + span)
        rows = pl.ds(seq * span, span)
        tail_rows = HALO // seq_count
        before = seq_count * span + seq * tail_rows
        rec_ref[first + HALO - tail_rows : first + HALO, :] = (
            rec_in[before : before + tail_rows] * kept
        )
        rec_ref[first + HALO : first + HALO + span, :] = rec_in[seq * span : (seq + 1) * span]
        kv = sums[seq * span : (seq + 1) * span, :kv_width]
        key = jnp.where(lane < head_dim, kv, 0.0)
        mean = jnp.sum(key * key, axis=-1, keepdims=True) * (1.0 / head_dim)
        scaled = kv * lax.rsqrt(mean + norm_eps) * key_gain
        message_ref[rows, :] = jnp.where(lane < head_dim, scaled, kv).astype(BF16)
        conv = jnp.zeros((span, channels), F32)
        for tap in range(CONV_TAPS):
            at = first + HALO - (CONV_TAPS - 1) + tap
            conv = conv + rec_ref[at : at + span, :] * taps[tap : tap + 1, :]
        conv = conv.astype(BF16)
        gated = jnp.dot(conv, gates_ref[...], preferred_element_type=F32)
        gate_decay, gate_input = gated[:, :channels], gated[:, channels:]
        log_decay = -lru_const * jax.nn.sigmoid(gate_decay) * rate + extra_ref[seq]
        decay = jnp.exp(log_decay)
        state = (
            jnp.sqrt(minus_expm1(2.0 * log_decay, decay * decay))
            * jax.nn.sigmoid(gate_input)
            * conv.astype(F32)
        )
        steps = 1
        while steps < span:
            state = state + decay * shifted_down(state, steps, 0.0)
            decay = decay * shifted_down(decay, steps, 1.0)
            steps *= 2
        state_ref[rows, :] = state
        decay_ref[rows, :] = decay
        for half in range(halves):
            lanes = slice(half * kv_width, (half + 1) * kv_width)
            at = seq * halves + half
            ends_ref[at : at + 1, :] = decay[span - 1 : span, lanes]
            at += seq_count * halves
            ends_ref[at : at + 1, :] = state[span - 1 : span, lanes]
    ends = ends_ref[...]
    high = ends.astype(BF16)
    left = ends - high.astype(F32)
    middle = left.astype(BF16)
    low = (left - middle.astype(F32)).astype(BF16)
    base = seq_count * span
    message_ref[base : base + 16, :] = jnp.concatenate([high, middle], axis=0)
    message_ref[base + 16 : base + 32, :] = jnp.concatenate([low, jnp.zeros_like(low)], axis=0)


def query_kernel(count, head_dim, seq_count, normed_ref, *refs):
    small_ref, query_ref = refs[-2:]
    width = query_ref.shape[2]
    span = query_ref.shape[1]
    heads = query_ref.shape[0] // seq_count
    gain = small_ref[QUERY_GAIN_ROW : QUERY_GAIN_ROW + 1, :width]
    sums = gathered_dot(normed_ref, refs[:-2], count)
    lane = lax.broadcasted_iota(jnp.int32, (span, width), 1)
    scaling = head_dim ** (-0.5)
    for seq in range(seq_count):
        rows = sums[seq * span : (seq + 1) * span]
        for head in range(heads):
            pair = rows[:, head // 2 * width : (head // 2 + 1) * width]
            if head % 2:
                pair = pltpu.roll(pair, head_dim, 1)
            own = jnp.where(lane < head_dim, pair, 0.0)
            mean = jnp.sum(own * own, axis=-1, keepdims=True) * (1.0 / head_dim)
            scaled = (own * lax.rsqrt(mean + norm_eps) * gain).astype(BF16)
            query_ref[seq * heads + head] = scaled * jnp.asarray(scaling, BF16)


def entering_kernel(count, group, *refs):
    place = lax.axis_index("sp")
    message_refs = refs[:count]
    (
        state_ref,
        decay_ref,
        normed_ref,
        part_ref,
        last_ref,
        small_ref,
        out_ref,
        ends_ref,
    ) = refs[count:]
    gate = gathered_dot(normed_ref, [last_ref], count, count - 1, part_ref[...])
    rows, channels = state_ref.shape
    width = ends_ref.shape[2]
    halves = channels // width
    seq_count = ends_ref.shape[1] // (2 * halves)
    span = rows // seq_count
    for index, message_ref in zip(arrivals(place, count), message_refs):
        parts = message_ref[rows:, :].astype(F32)
        ends_ref[index] = parts[0:8] + parts[8:16] + parts[16:24]
    half_rows = seq_count * halves
    entering = jnp.zeros((half_rows, width), F32)
    for earlier in range(count - 1):
        ends = ends_ref[earlier]
        merged = ends[:half_rows] * entering + ends[half_rows:]
        entering = jnp.where(earlier < place, merged, entering)
    lane = lax.broadcasted_iota(jnp.int32, (span, width), 1)
    for seq in range(seq_count):
        for half in range(halves):
            lanes = slice(half * width, (half + 1) * width)
            at = seq * halves + half
            part = pl.ds(seq * span, span)
            first = seq * span
            state = state_ref[part, lanes] + decay_ref[part, lanes] * entering[at : at + 1, :]
            gated = state * jax.nn.gelu(gate[first : first + span, lanes])
            square = gated * gated
            total = jnp.sum(square, axis=-1, keepdims=True)
            low = jnp.sum(jnp.where(lane < group, square, 0.0), axis=-1, keepdims=True)
            mean = jnp.where(lane < group, low, total - low) * (1.0 / group)
            out_ref[part, lanes] = (
                gated * lax.rsqrt(mean + norm_eps) * small_ref[REC_GAIN_ROW : REC_GAIN_ROW + 1, lanes]
            ).astype(BF16)


def lane_sums(value, first=0):
    lanes = value.shape[1]
    row = lax.broadcasted_iota(jnp.int32, (lanes, lanes), 0)
    chosen = jnp.where(row >= first, 1.0, 0.0).astype(BF16)
    high = value.astype(BF16)
    low = (value - high.astype(F32)).astype(BF16)
    return jnp.dot(high, chosen, preferred_element_type=F32) + jnp.dot(
        low, chosen, preferred_element_type=F32
    )


def attention_kernel(count, head_dim, first, last, *refs):
    query_ref = refs[0]
    message_refs = refs[1 : 1 + last - first]
    refs = refs[1 + last - first :]
    gate_ref = refs[0]
    before_refs = refs[1:4] if first else None
    score_ref = refs[-1]
    if last == count:
        small_ref, out_ref = refs[-3:-1]
    else:
        after_refs = refs[-4:-1]
    span, width = query_ref.shape[1:]
    seq_count = gate_ref.shape[0]
    heads = query_ref.shape[0] // seq_count
    place = lax.axis_index("sp")
    found = arrivals(place, count)[first:last]
    ahead = lax.broadcasted_iota(jnp.int32, (span, span), 1) - lax.broadcasted_iota(
        jnp.int32, (span, span), 0
    )
    lane = lax.broadcasted_iota(jnp.int32, (span, width), 1)
    for seq in range(seq_count):
        keys = pl.ds(seq * span, span)
        lines = [
            slice((seq * heads + head) * span, (seq * heads + head + 1) * span)
            for head in range(heads)
        ]
        queries = query_ref[seq * heads : (seq + 1) * heads].reshape(heads * span, width)
        top = [None] * heads
        own = gate_ref[seq, :, pl.ds(pl.multiple_of(place * span, span), span)]
        own = jnp.concatenate([own, jnp.zeros((span - heads, span), F32)], axis=0).T
        for at, block in enumerate(found):
            scores = lax.dot_general(
                queries,
                message_refs[at][keys, :],
                (((1,), (1,)), ((), ())),
                preferred_element_type=F32,
            )
            hidden = ahead > (place - block) * span
            gates = gate_ref[seq, :, pl.ds(pl.multiple_of(block * span, span), span)]
            for head in range(heads):
                score = scores[head * span : (head + 1) * span]
                score = score + own[:, head : head + 1] - gates[head : head + 1, :]
                score = jnp.where(hidden, -jnp.inf, score)
                score_ref[at, head * span : (head + 1) * span, :] = score
                top[head] = score if at == 0 else jnp.maximum(top[head], score)
        top = [jnp.max(part, axis=-1, keepdims=True) for part in top]
        if first:
            top_before = [before_refs[0][line, :] for line in lines]
            top = [jnp.maximum(part, old) for part, old in zip(top, top_before)]
        totals = [None] * heads
        weighted = None
        for at in range(len(found)):
            weights = []
            for head in range(heads):
                part = jnp.exp(score_ref[at, head * span : (head + 1) * span, :] - top[head])
                totals[head] = part if at == 0 else totals[head] + part
                weights.append(part.astype(BF16))
            term = jnp.dot(
                jnp.concatenate(weights, axis=0),
                message_refs[at][keys, :],
                preferred_element_type=F32,
            )
            weighted = term if at == 0 else weighted + term
        outs = []
        for head in range(heads):
            total = lane_sums(totals[head])
            value = weighted[head * span : (head + 1) * span]
            line = lines[head]
            if first:
                fading = jnp.exp(top_before[head] - top[head])
                total = total + before_refs[1][line, :] * fading
                value = value + before_refs[2][line, :] * fading
            if last < count:
                after_refs[0][line, :] = jnp.broadcast_to(top[head], value.shape)
                after_refs[1][line, :] = total
                after_refs[2][line, :] = value
                continue
            mean = lane_sums(value * value, head_dim) * (1.0 / head_dim)
            outs.append(value * lax.rsqrt(mean + norm_eps * (total * total)))
        for pair in range(len(outs) // 2):
            lanes = slice(pair * width, (pair + 1) * width)
            joined = jnp.where(
                lane < head_dim, pltpu.roll(outs[2 * pair], head_dim, 1), outs[2 * pair + 1]
            )
            gain = small_ref[ATT_GAIN_ROW : ATT_GAIN_ROW + 1, lanes]
            out_ref[keys, lanes] = (joined * gain).astype(BF16)


def output_kernel(uses, has_base, *refs):
    out_ref = refs[-1]
    total = refs[-2][...] if has_base else None
    for left, right, half in uses:
        rows = refs[left].shape[1]
        term = jnp.dot(
            refs[left][...],
            refs[right][half * rows : (half + 1) * rows, :],
            preferred_element_type=F32,
        )
        total = term if total is None else total + term
    out_ref[...] = total.astype(out_ref.dtype)


def tp_spread(value, count):
    bits = [1 << at for at in range(count.bit_length() - 1)]
    found = {0: value}
    for bit in reversed(bits):
        pairs = [(source, source ^ bit) for source in range(count)]
        for member in sorted(found):
            found[member ^ bit] = lax.ppermute(found[member], "tp", pairs)
    return [found[member] for member in range(count)]


def ring_body(
    inputs,
    norm_gain,
    query_weight,
    key_weight,
    value_weight,
    query_gain,
    key_gain,
    forget_cache,
    rec_in_weight,
    rec_gate_weight,
    conv_weight,
    decay_gate_weight,
    input_gate_weight,
    decay_param,
    decay_extra,
    attn_out_gain,
    rec_out_gain,
    out_att_weight,
    out_rec_weight,
):
    count = lax.axis_size("sp")
    tp_count = lax.axis_size("tp")
    seq_count, span, model_width = inputs.shape
    rows = seq_count * span
    head_dim = query_gain.shape[0]
    width = 2 * head_dim
    att_width = query_weight.shape[1]
    heads = att_width // head_dim
    channels = rec_in_weight.shape[1]
    ext_rows = seq_count * (HALO + span)
    out_cols = model_width // tp_count
    query_ring = Ring(query_weight, count, False)
    query_ring.step(1)
    begun = call(begin_kernel, jax.ShapeDtypeStruct((8, 128), F32), [], flops=BEGIN_FLOPS)
    first_chunk = call(
        pack_kernel,
        jax.ShapeDtypeStruct((rec_in_weight.shape[0], width + channels), BF16),
        [begun, key_weight.T, value_weight.T, rec_in_weight],
    )
    first_ring = Ring(first_chunk, count, True)
    first_ring.step(1)
    slice_width = model_width // count
    normed, tail, gate_weights, small = call(
        norm_kernel,
        [
            jax.ShapeDtypeStruct((count, rows, slice_width), BF16),
            jax.ShapeDtypeStruct((count, HALO, slice_width), BF16),
            jax.ShapeDtypeStruct((channels, 2 * channels), BF16),
            jax.ShapeDtypeStruct((16, channels), F32),
        ],
        [
            inputs,
            norm_gain.reshape(1, model_width),
            decay_gate_weight,
            input_gate_weight,
            conv_weight,
            decay_param.reshape(1, channels),
            rec_out_gain.reshape(1, channels),
            attn_out_gain.reshape(1, att_width),
            key_gain.reshape(1, head_dim),
            query_gain.reshape(1, head_dim),
        ],
    )
    out_weight = list(
        call(
            pack_out_kernel,
            [jax.ShapeDtypeStruct((att_width + channels, out_cols), BF16)] * tp_count,
            [out_att_weight, out_rec_weight],
        )
    )
    shift = [(member, (member + 1) % count) for member in range(count)]
    halo = lax.ppermute(tail, "sp", shift)
    for member in range(1, tp_count):
        pairs = [(source, source ^ member) for source in range(tp_count)]
        out_weight[member] = lax.ppermute(out_weight[member], "tp", pairs)

    for number in range(2, count // 2 + 1):
        first_ring.step(number)
        query_ring.step(number)
    gate_ring = Ring(rec_gate_weight, count, False)
    for number in range(1, count // 2 + 1):
        gate_ring.step(number)

    def part_of(ring, halos=()):
        columns = ring.blocks[0].shape[1]
        return call(
            functools.partial(part_kernel, count, len(halos)),
            jax.ShapeDtypeStruct((rows + len(halos) * HALO, columns), F32),
            [normed, *halos, *ring.blocks[:-1]],
        )

    message, local_state, cum_decay = call(
        functools.partial(recurrence_kernel, count, head_dim),
        [
            jax.ShapeDtypeStruct((rows + STATE_ROWS, width), BF16),
            jax.ShapeDtypeStruct((rows, channels), F32),
            jax.ShapeDtypeStruct((rows, channels), F32),
        ],
        [
            normed,
            halo,
            part_of(first_ring, (halo,)),
            first_ring.blocks[-1],
            small,
            gate_weights,
            decay_extra,
        ],
        scratch=[pltpu.VMEM((ext_rows, channels), F32), pltpu.VMEM((8, width), F32)],
    )
    message_ring = Ring(message, count, True)
    for number in range(1, count // 2 + 1):
        message_ring.step(number)

    queries = call(
        functools.partial(query_kernel, count, head_dim, seq_count),
        jax.ShapeDtypeStruct((seq_count * heads, span, width), BF16),
        [normed, *query_ring.blocks, small],
    )
    messages = message_ring.blocks
    rec_normed = call(
        functools.partial(entering_kernel, count, LRU_BLOCK),
        jax.ShapeDtypeStruct((rows, channels), BF16),
        [
            *messages,
            local_state,
            cum_decay,
            normed,
            part_of(gate_ring),
            gate_ring.blocks[-1],
            small,
        ],
        scratch=[pltpu.VMEM((count, 8, width), F32)],
    )
    early = count - 1
    attended = call(
        functools.partial(attention_kernel, count, head_dim, 0, early),
        [jax.ShapeDtypeStruct((seq_count * heads * span, width), F32)] * 3,
        [queries, *messages[:early], forget_cache],
        scratch=[pltpu.VMEM((early, heads * span, span), F32)],
    )
    att_normed = call(
        functools.partial(attention_kernel, count, head_dim, early, count),
        jax.ShapeDtypeStruct((rows, att_width), BF16),
        [queries, *messages[early:], forget_cache, *attended, small],
        scratch=[pltpu.VMEM((count - early, heads * span, span), F32)],
    )

    def project(rec_members, att_members, base, kind):
        operands, uses = [], []
        weights = sorted({*rec_members, *att_members})
        for parts, half, members in ((rec_parts, 1, rec_members), (att_parts, 0, att_members)):
            for member in members:
                uses.append((len(operands), -1 - member, half))
                operands.append(parts[member])
        at_weight = {member: len(operands) + at for at, member in enumerate(weights)}
        uses = [(left, at_weight[-1 - right], half) for left, right, half in uses]
        operands += [out_weight[member] for member in weights]
        if base is not None:
            operands.append(base)
        return call(
            functools.partial(output_kernel, tuple(uses), base is not None),
            jax.ShapeDtypeStruct((rows, out_cols), kind),
            operands,
        )

    rec_parts = tp_spread(rec_normed, tp_count)
    att_parts = tp_spread(att_normed, tp_count)
    near, far = range(tp_count // 2), range(tp_count // 2, tp_count)
    base = project(range(tp_count), near, None, F32)
    if len(far) > 1:
        base = project((), far[:1], base, F32)
    mixed = project((), far[-1:], base, BF16)
    return mixed.reshape(seq_count, span, out_cols)


def fits(count, tp_count):
    return 4 <= count <= 16 and count % 2 == 0 and tp_count in (2, 4)


def layer(*arrays):
    inputs, query_weight, key_weight = arrays[0], arrays[2], arrays[3]
    head_dim, rec_in_weight = arrays[5].shape[0], arrays[8]
    count, tp_count = lax.axis_size("sp"), lax.axis_size("tp")
    whole_blocks = (
        inputs.shape[0] == 2
        and rec_in_weight.shape[1] == 4 * head_dim
        and inputs.shape[1] == 2 * head_dim
        and key_weight.shape[1] == head_dim
        and query_weight.shape[1] == rec_in_weight.shape[1]
        and inputs.shape[2] % (128 * count) == 0
    )
    return (ring_body if fits(count, tp_count) and whole_blocks else body)(*arrays)


def solution(mesh):
    return jax.shard_map(
        layer,
        mesh=mesh,
        in_specs=(
            P(None, "sp", None),
            P(),
            P("sp", "tp"),
            P("sp", "tp"),
            P("sp", "tp"),
            P(),
            P(),
            P(None, "tp", None),
            P("sp", "tp"),
            P("sp", "tp"),
            P(None, "tp"),
            P("tp", None, None),
            P("tp", None, None),
            P("tp"),
            P(None, "sp", "tp"),
            P("tp"),
            P("tp"),
            P("tp", None),
            P("tp", None),
        ),
        out_specs=P(None, "sp", "tp"),
        check_vma=False,
    )
```
